32 devices in a mesh: sp: 8 (over z, x), tp: 4 (over y, core).
Axes of the slice: x: 2, y: 2, z: 4, core: 2. Of those that a mesh axis runs over, the one named last changes fastest.
Arguments:
- x_in: bfloat16 [4096, 1024], P('sp', 'tp'), may hold values from -6 to 6
- gate_b: bfloat16 [4096, 1024], P('sp', 'tp'), may hold values from -6 to 6
- gate_c: bfloat16 [4096, 1024], P('sp', 'tp'), may hold values from -6 to 6
- conv_taps: bfloat16 [3, 1024], P(None, 'tp'), may hold values from -3.5 to 3.5
- out_proj: bfloat16 [1024, 2048], P('tp'), may hold values from -0.1875 to 0.1875
- mix_gain: bfloat16 [2048], replicated, may hold values from 0.099609375 to 1.8984375
- resid: bfloat16 [4096, 2048], P(('sp', 'tp')), may hold values from -6 to 6
- pre_gain: bfloat16 [2048], replicated, may hold values from 0.099609375 to 1.8984375
- expert_gate: bfloat16 [8, 2048, 512], P('sp'), may hold values from -0.125 to 0.125
- expert_up: bfloat16 [8, 2048, 512], P('sp'), may hold values from -0.125 to 0.125
- expert_down: bfloat16 [8, 512, 2048], P('sp'), may hold values from -7.1594562 to 7.1594562
- shared_gate: bfloat16 [2048, 256], replicated, may hold values from -0.125 to 0.125
- shared_up: bfloat16 [2048, 256], replicated, may hold values from -0.125 to 0.125
- shared_down: bfloat16 [256, 2048], replicated, may hold values from -10.125 to 10.125
- post_gain: bfloat16 [2048], replicated, may hold values from 0.099609375 to 1.8984375
- routes: int32 [4096, 4], P(('sp', 'tp')), may hold values from 0 to 7, all different within a row; in each aligned block of 128 rows (0 to 127, 128 to 255, ...) at most 96 rows name the same one
- route_weights: float32 [4096, 4], P(('sp', 'tp')), may hold values from 0.1 to 1
Outputs:
- layer_out: bfloat16 [4096, 2048], P(('sp', 'tp'))
The draws below stay inside these ranges and needn't reach their ends.
Inputs may be any that keep to these rules, and one draw needn't show every extreme that they name: `routes`: each row names 4 different experts. Within the rows of one device (aligned blocks), no expert is named by more than 96 rows, and in some block one expert is named by exactly 96 rows.
All inputs are finite; a program needn't handle non-finite values.
Results may differ from the reference program's by a relative error of at most 0.007.
Values may be sent and summed in bfloat16 or wider, within the bound.
No kernel may reach another device: no remote copies, remote signals or barrier semaphores. Data moves between devices by JAX's collectives and lax.ppermute only.
A program may use at most 128 MiB of HBM per device.

```python
import math
import jax
import jax.numpy as jnp
import numpy as np
from jax import lax

D = 2048
CONV_CH = 1024
EXPERT_HIDDEN = 512
SHARED_HIDDEN = 256
CONV_WIDTH = 3
TOPK = 4
TOK_DEV = 512
EXPERTS = 8
CAP = 96
TOKENS = 4096
N_SP = 8
N_TP = 4


def column_scale(key, count):
    ramp = 3.0 ** (jnp.arange(count, dtype=jnp.float32) / count)
    rough = 10.0 ** jax.random.uniform(key, (count,), jnp.float32)
    return ramp * rough / 10.0


def draw_expert_down(key, part):
    first, second = jax.random.split(key)
    base = jnp.clip(jax.random.normal(first, (EXPERTS, EXPERT_HIDDEN, D), jnp.float32), -6.0, 6.0)
    return (base * EXPERT_HIDDEN ** (-0.5) * column_scale(second, D)[None, None, :]).astype(jnp.bfloat16)


def draw_shared_down(key, part):
    first, second = jax.random.split(key)
    base = jnp.clip(jax.random.normal(first, (SHARED_HIDDEN, D), jnp.float32), -6.0, 6.0)
    return (base * SHARED_HIDDEN ** (-0.5) * column_scale(second, D)[None, :]).astype(jnp.bfloat16)


def levels(rng, dims, shards, low, top_value):
    gain, own = 1.0, jax.random.fold_in(rng, 6)
    for dim, blocks in shards:
        steps = jnp.exp(jax.random.uniform(jax.random.fold_in(own, dim), (blocks,), jnp.float32, low / len(shards), top_value / len(shards)))
        gain = gain * jnp.repeat(steps, dims[dim] // blocks).reshape([-1 if axis == dim else 1 for axis in range(len(dims))])
    return gain


def assign_block(stream_key, own, number, rows, number_of, top, most, skew):
    order = jax.random.permutation(stream_key, number_of)
    packed, common = load_shares(number_of, rows * top, most, skew, True), load_shares(number_of, rows * top, most, skew, False)
    places = jnp.arange(number_of)

    def named(tallies, rotation):
        used = int((tallies > 0).sum())
        fixed = max(1, used // 4)
        moved = fixed + (places - fixed + rotation * (used - fixed)) % max(1, number_of - fixed)
        return jnp.zeros((number_of,), jnp.int32).at[order[jnp.where(places < fixed, places, moved)]].set(jnp.asarray(tallies, jnp.int32))

    tallies = jnp.where(number % 4 == 0, named(packed, number // 4), named(common, number - number // 4 - 1))
    mixed = jax.random.permutation(jax.random.fold_in(own, 3), number_of)
    giver, sink = mixed[0:number_of // 2 * 2:2], mixed[1:number_of // 2 * 2:2]
    margin = jnp.minimum(tallies[giver] - 1, most - tallies[sink]) // 2
    margin = jnp.where((giver == order[0]) | (sink == order[0]) | (tallies[sink] == 0), 0, jnp.maximum(margin, 0))
    moved = jax.random.randint(jax.random.fold_in(own, 4), (number_of // 2,), 0, 1 << 20) % (margin + 1)
    tallies = tallies.at[giver].add(-moved).at[sink].add(moved)
    members = jnp.searchsorted(jnp.cumsum(tallies), jnp.arange(rows * top), side="right").astype(jnp.int32)
    table = members.reshape(top, rows).T
    table = table[jax.random.permutation(jax.random.fold_in(own, 1), rows)]
    rotation = jax.random.randint(jax.random.fold_in(own, 2), (rows, 1), 0, top)
    return jnp.take_along_axis(table, (jnp.arange(top)[None, :] + rotation) % top, axis=1)


def load_shares(count, total, bound, lean, full):
    loads = [(1 << 20) // math.isqrt(grade ** lean) + 1 for grade in range(1, count + 1)]
    largest = bound if full else min(bound, max(-(-total // count), total * loads[0] // sum(loads)))
    least = 1 if total - largest >= count - 1 else 0
    holding, rest = [largest] + [least] * (count - 1), total - largest - least * (count - 1)
    while rest > 0:
        free = [i for i in range(1, count) if holding[i] < largest] or [i for i in range(1, count) if holding[i] < bound]
        whole, budget = sum([loads[i] for i in free]), rest
        for i in free:
            addition = min(bound - holding[i], max(1, budget * loads[i] // whole), rest)
            holding[i] = holding[i] + addition
            rest = rest - addition
    return np.array(holding)


def centred(own_key, extent, spread, most, pieces=(), kind=jnp.bfloat16):
    level = levels(own_key, extent, pieces, -0.22, 0.18) if pieces else 1.0
    array = jax.random.normal(own_key, extent, jnp.float32) * spread * level
    return jnp.minimum(jnp.maximum(array, -most), most).astype(kind)


def setup_inputs(seed: int = 0) -> dict:
    arg_keys = jax.random.split(jax.random.key(seed), 18)
    x_in = centred(arg_keys[0], (TOKENS, CONV_CH), 1.0, 6.0, ((0, 8), (1, 4)))
    gate_b = centred(arg_keys[1], (TOKENS, CONV_CH), 1.0, 6.0, ((0, 8), (1, 4)))
    gate_c = centred(arg_keys[2], (TOKENS, CONV_CH), 1.0, 6.0, ((0, 8), (1, 4)))
    conv_taps = centred(arg_keys[3], (CONV_WIDTH, CONV_CH), CONV_WIDTH ** -0.5, 3.5, ((1, 4),))
    out_proj = centred(arg_keys[4], (CONV_CH, D), CONV_CH ** -0.5, 0.1875, ((0, 4),))
    mix_gain = jnp.clip(1.0 + 0.18 * jax.random.normal(arg_keys[5], (D,), jnp.float32), 0.099609375, 1.8984375).astype(jnp.bfloat16)
    resid = centred(arg_keys[6], (TOKENS, D), 1.0, 6.0, ((0, 32),))
    pre_gain = jnp.clip(1.0 + 0.18 * jax.random.normal(arg_keys[7], (D,), jnp.float32), 0.099609375, 1.8984375).astype(jnp.bfloat16)
    expert_gate = centred(arg_keys[8], (EXPERTS, D, EXPERT_HIDDEN), D ** -0.5, 0.125, ((0, 8),))
    expert_up = centred(arg_keys[9], (EXPERTS, D, EXPERT_HIDDEN), D ** -0.5, 0.125, ((0, 8),))
    expert_down = draw_expert_down(jax.random.fold_in(arg_keys[17], 71), 0)
    shared_gate = centred(arg_keys[11], (D, SHARED_HIDDEN), D ** -0.5, 0.125)
    shared_up = centred(arg_keys[12], (D, SHARED_HIDDEN), D ** -0.5, 0.125)
    shared_down = draw_shared_down(jax.random.fold_in(arg_keys[17], 71), 0)
    post_gain = jnp.clip(1.0 + 0.18 * jax.random.normal(arg_keys[14], (D,), jnp.float32), 0.099609375, 1.8984375).astype(jnp.bfloat16)
    routes_keys = jax.random.split(jax.random.fold_in(arg_keys[15], 1), TOKENS // (TOK_DEV // N_TP))
    routes_turns = jax.random.permutation(jax.random.fold_in(arg_keys[15], 3), TOKENS // (TOK_DEV // N_TP))
    routes = jax.vmap(lambda own, number: assign_block(jax.random.fold_in(arg_keys[15], 2), own, number, TOK_DEV // N_TP, EXPERTS, TOPK, CAP, 2))(routes_keys, routes_turns).reshape((TOKENS, TOPK))
    route_weights = jnp.clip(0.1 + 0.9 * jax.random.uniform(arg_keys[16], (TOKENS, TOPK), jnp.float32) ** levels(arg_keys[16], (TOKENS, TOPK), ((0, 32),), -0.2, 0.2), 0.1, 1.0)
    return dict(x_in=x_in, gate_b=gate_b, gate_c=gate_c, conv_taps=conv_taps, out_proj=out_proj, mix_gain=mix_gain, resid=resid, pre_gain=pre_gain, expert_gate=expert_gate, expert_up=expert_up, expert_down=expert_down, shared_gate=shared_gate, shared_up=shared_up, shared_down=shared_down, post_gain=post_gain, routes=routes, route_weights=route_weights)


epsilon = 1e-06

def reference(x_in, gate_b, gate_c, conv_taps, out_proj, mix_gain, resid, pre_gain, expert_gate, expert_up, expert_down, shared_gate, shared_up, shared_down, post_gain, routes, route_weights):
    mixed_in = gate_c.astype(jnp.float32) * x_in.astype(jnp.float32)
    reach = CONV_WIDTH - 1
    padded = jnp.concatenate([jnp.zeros((reach, CONV_CH), jnp.float32), mixed_in], 0)
    taps = conv_taps.astype(jnp.float32)
    convolved = jnp.zeros((TOKENS, CONV_CH), jnp.float32)
    for index in range(CONV_WIDTH):
        convolved = convolved + taps[index][None, :] * padded[index:index + TOKENS]
    conv_out = (gate_b.astype(jnp.float32) * convolved).astype(jnp.bfloat16)
    projected = jnp.dot(conv_out, out_proj, preferred_element_type=jnp.float32)
    row_scale = lax.rsqrt(lax.optimization_barrier(jnp.mean(projected * projected, axis=1, keepdims=True)) + epsilon)
    resid1 = (resid.astype(jnp.float32) + projected * row_scale * mix_gain.astype(jnp.float32)).astype(jnp.bfloat16)
    wide_resid = resid1.astype(jnp.float32)
    normed = (wide_resid * lax.rsqrt(lax.optimization_barrier(jnp.mean(wide_resid * wide_resid, axis=1, keepdims=True)) + epsilon) * pre_gain.astype(jnp.float32)).astype(jnp.bfloat16)
    block_count = N_SP * N_TP
    quarter = TOK_DEV // N_TP
    flat_ids = routes.reshape(-1).astype(jnp.int32)
    onehot = (flat_ids[:, None] == jnp.arange(EXPERTS, dtype=jnp.int32)[None, :]).astype(jnp.int32)
    blocks = onehot.reshape(block_count, quarter * TOPK, EXPERTS)
    before = (jnp.cumsum(blocks, axis=1) - blocks).reshape(-1, EXPERTS)
    position = lax.optimization_barrier(jnp.sum(before * onehot, axis=1))
    source = jnp.arange(TOKENS * TOPK, dtype=jnp.int32) // (quarter * TOPK)
    slot_index = flat_ids * (block_count * CAP) + source * CAP + position
    dispatched = jnp.zeros((EXPERTS * block_count * CAP, D), jnp.bfloat16).at[slot_index].set(jnp.repeat(normed, TOPK, axis=0))

    def run_expert(operands):
        rows_in, w_gate, w_up, w_down = operands
        gate_h = jnp.dot(rows_in, w_gate, preferred_element_type=jnp.float32)
        up_h = jnp.dot(rows_in, w_up, preferred_element_type=jnp.float32)
        hidden = (jax.nn.silu(gate_h) * up_h).astype(jnp.bfloat16)
        return jnp.dot(hidden, w_down, preferred_element_type=jnp.float32).astype(jnp.bfloat16)
    expert_out = lax.map(run_expert, (dispatched.reshape(EXPERTS, block_count * CAP, D), expert_gate, expert_up, expert_down)).reshape(-1, D)
    picked = expert_out[slot_index].reshape(TOKENS, TOPK, D)
    routed = jnp.zeros((TOKENS, D), jnp.float32)
    for index in range(TOPK):
        routed = routed + route_weights[:, index:index + 1] * picked[:, index].astype(jnp.float32)
    shared_g = jnp.dot(normed, shared_gate, preferred_element_type=jnp.float32)
    shared_u = jnp.dot(normed, shared_up, preferred_element_type=jnp.float32)
    shared_hidden = (jax.nn.silu(shared_g) * shared_u).astype(jnp.bfloat16)
    shared_out = jnp.dot(shared_hidden, shared_down, preferred_element_type=jnp.float32)
    branch = routed + shared_out
    factor = lax.rsqrt(lax.optimization_barrier(jnp.mean(branch * branch, axis=1, keepdims=True)) + epsilon)
    return (wide_resid + branch * factor * post_gain.astype(jnp.float32)).astype(jnp.bfloat16)
```

```python
import jax
import jax.numpy as jnp
from jax import lax
from jax.sharding import PartitionSpec as P

epsilon = 1e-06
f32 = jnp.float32
bf16 = jnp.bfloat16


def passed_along(shard, axis, by):
    size = lax.axis_size(axis)
    pairs = [(i, i + by) for i in range(size) if 0 <= i + by < size]
    return lax.ppermute(shard, axis, pairs)


def routed_body(
    x_in,
    gate_b,
    gate_c,
    conv_taps,
    out_proj,
    mix_gain,
    resid,
    pre_gain,
    expert_gate,
    expert_up,
    expert_down,
    shared_gate,
    shared_up,
    shared_down,
    post_gain,
    routes,
    route_weights,
):
    row_count = x_in.shape[0]
    channels = x_in.shape[1]
    reach = conv_taps.shape[0] - 1
    edge_rows = jnp.concatenate([x_in[row_count - reach :], gate_c[row_count - reach :]], 1)
    arrived_edge = passed_along(edge_rows, "sp", 1)
    inputs = jnp.concatenate([arrived_edge[:, :channels], x_in], 0).astype(jnp.float32)
    gate_rows = jnp.concatenate([arrived_edge[:, channels:], gate_c], 0).astype(jnp.float32)
    mixed_in = inputs * gate_rows
    taps = conv_taps.astype(jnp.float32)
    convolved = jnp.zeros((row_count, channels), jnp.float32)
    for index in range(reach + 1):
        convolved = convolved + taps[index][None, :] * mixed_in[index : index + row_count]
    conv_out = (gate_b.astype(jnp.float32) * convolved).astype(jnp.bfloat16)
    width_all = out_proj.shape[1]
    full_rows = lax.all_to_all(conv_out, "tp", split_axis=0, concat_axis=1, tiled=True)
    projected = jnp.dot(
        full_rows,
        lax.all_gather(out_proj, "tp", axis=0, tiled=True),
        preferred_element_type=jnp.float32,
    )
    row_scale = lax.rsqrt(jnp.mean(projected * projected, axis=1, keepdims=True) + epsilon)
    resid1 = (
        resid.astype(jnp.float32) + projected * row_scale * mix_gain.astype(jnp.float32)
    ).astype(jnp.bfloat16)
    wide_resid = resid1.astype(jnp.float32)
    normed = (
        wide_resid
        * lax.rsqrt(jnp.mean(wide_resid * wide_resid, axis=1, keepdims=True) + epsilon)
        * pre_gain.astype(jnp.float32)
    ).astype(jnp.bfloat16)
    experts = lax.axis_size("sp")
    local_rows = resid.shape[0]
    top_count = routes.shape[1]
    capacity = 3 * local_rows * top_count // (2 * experts)
    flat_ids = routes.reshape(-1)
    onehot = (flat_ids[:, None] == jnp.arange(experts, dtype=jnp.int32)[None, :]).astype(jnp.int32)
    before = jnp.cumsum(onehot, axis=0) - onehot
    position = jnp.sum(before * onehot, axis=1)
    slot_index = flat_ids * capacity + position
    outgoing = (
        jnp.zeros((experts * capacity, width_all), jnp.bfloat16)
        .at[slot_index]
        .set(jnp.repeat(normed, top_count, axis=0))
    )
    received = lax.all_to_all(
        outgoing.reshape(experts, capacity, width_all),
        "sp",
        split_axis=0,
        concat_axis=0,
        tiled=True,
    )
    arrived = received.reshape(experts * capacity, width_all)
    gate_h = jnp.dot(arrived, expert_gate[0], preferred_element_type=jnp.float32)
    up_h = jnp.dot(arrived, expert_up[0], preferred_element_type=jnp.float32)
    hidden = (jax.nn.silu(gate_h) * up_h).astype(jnp.bfloat16)
    expert_out = jnp.dot(hidden, expert_down[0], preferred_element_type=jnp.float32).astype(
        jnp.bfloat16
    )
    returned = lax.all_to_all(
        expert_out.reshape(experts, capacity, width_all),
        "sp",
        split_axis=0,
        concat_axis=0,
        tiled=True,
    )
    returned = returned.reshape(experts * capacity, width_all)
    picked = returned[slot_index].astype(jnp.float32).reshape(local_rows, top_count, width_all)
    routed = jnp.einsum("tk,tkd->td", route_weights, picked)
    shared_g = jnp.dot(normed, shared_gate, preferred_element_type=jnp.float32)
    shared_u = jnp.dot(normed, shared_up, preferred_element_type=jnp.float32)
    shared_hidden = (jax.nn.silu(shared_g) * shared_u).astype(jnp.bfloat16)
    shared_out = jnp.dot(shared_hidden, shared_down, preferred_element_type=jnp.float32)
    branch = routed + shared_out
    factor = lax.rsqrt(jnp.mean(branch * branch, axis=1, keepdims=True) + epsilon)
    return (wide_resid + branch * factor * post_gain.astype(jnp.float32)[None, :]).astype(
        jnp.bfloat16
    )


def dot(a, b):
    return jnp.dot(a, b, preferred_element_type=f32)


def flip(array, axis, bit):
    return lax.ppermute(array, axis, [(i, i ^ bit) for i in range(lax.axis_size(axis))])


def along_z(array, moves):
    pairs = [(2 * a + x, 2 * b + x) for a, b in moves for x in range(2)]
    return lax.ppermute(array, "sp", pairs)


UP = [(0, 1), (1, 2), (2, 3)]
DOWN = [(1, 0), (2, 1), (3, 2)]


def pick(index, arrays):
    out = arrays[-1]
    for i in range(len(arrays) - 2, -1, -1):
        out = jnp.where(index == i, arrays[i], out)
    return out


def dense_body(
    x_in,
    gate_b,
    gate_c,
    conv_taps,
    out_proj,
    mix_gain,
    resid,
    pre_gain,
    expert_gate,
    expert_up,
    expert_down,
    shared_gate,
    shared_up,
    shared_down,
    post_gain,
    routes,
    route_weights,
):
    s = lax.axis_index("sp")
    t = lax.axis_index("tp")
    z, y, c = s // 2, t // 2, t % 2
    experts = lax.axis_size("sp")
    tp_size = lax.axis_size("tp")
    rows = resid.shape[0]
    row_count, channels = x_in.shape
    reach = conv_taps.shape[0] - 1
    edge = 8

    mixed_in = gate_c.astype(f32) * x_in.astype(f32)
    edge_in = passed_along(mixed_in[row_count - edge :], "sp", 1)

    lanes = jnp.arange(experts, dtype=jnp.int32)
    dense_w = jnp.sum(
        jnp.where(routes[None] == lanes[:, None, None], route_weights[None], 0.0), axis=2
    )
    pair_w = jnp.stack([dense_w, dense_w.reshape(experts // 2, 2, rows)[:, ::-1].reshape(experts, rows)], 1)
    all_w = lax.all_to_all(pair_w, "sp", split_axis=0, concat_axis=0, tiled=True)
    all_w = all_w.reshape(experts // 2, 2, 2, rows)
    line_w = pick(s % 2, [all_w[:, 0], all_w[:, 1]])

    proj_other = flip(out_proj, "tp", 1)

    gate_w, up_w, down_w = expert_gate[0], expert_up[0], expert_down[0]
    part = gate_w.shape[1] // tp_size
    gu_part = pick(
        t,
        [
            jnp.concatenate(
                [gate_w[:, i * part : (i + 1) * part], up_w[:, i * part : (i + 1) * part]], 1
            )
            for i in range(tp_size)
        ],
    )
    down_part = pick(t, [down_w[i * part : (i + 1) * part] for i in range(tp_size)])
    gu_a = flip(gu_part, "sp", 1)
    down_a = flip(down_part, "sp", 1)

    padded = jnp.concatenate([edge_in, mixed_in], 0)
    taps = conv_taps.astype(f32)
    convolved = jnp.zeros((row_count, channels), f32)
    for index in range(reach + 1):
        start = edge - reach + index
        convolved = convolved + taps[index][None, :] * padded[start : start + row_count]
    conv_out = (gate_b.astype(f32) * convolved).astype(bf16)

    blocks = conv_out.reshape(2, 2, rows, channels)
    mine = pick(c, [blocks[:, 0], blocks[:, 1]])
    give = pick(c, [blocks[:, 1], blocks[:, 0]])
    got = flip(give, "tp", 1)
    far = dot(pick(y, [mine[1], mine[0]]), out_proj) + dot(pick(y, [got[1], got[0]]), proj_other)
    far_in = flip(far.astype(bf16), "tp", 2)
    near = dot(pick(y, [mine[0], mine[1]]), out_proj) + dot(pick(y, [got[0], got[1]]), proj_other)
    projected = near + far_in.astype(f32)

    gu_b = flip(gu_a, "tp", 2)
    down_b = flip(down_a, "tp", 2)

    row_scale = lax.rsqrt(jnp.mean(projected * projected, axis=1, keepdims=True) + epsilon)
    resid1 = (resid.astype(f32) + projected * row_scale * mix_gain.astype(f32)).astype(bf16)
    wide_resid = resid1.astype(f32)
    normed = (
        wide_resid
        * lax.rsqrt(jnp.mean(wide_resid * wide_resid, axis=1, keepdims=True) + epsilon)
        * pre_gain.astype(f32)
    ).astype(bf16)

    below1 = along_z(normed, UP)
    above1 = along_z(normed, DOWN)
    below2 = along_z(below1, UP[1:])
    above2 = along_z(above1, DOWN[:2])
    two = jnp.where(z >= 2, below2, above2)
    three = along_z(two, [(2, 3), (1, 0)])

    gu_ab = jnp.concatenate([gu_a, gu_b], 1)
    gu_other = jnp.concatenate([gu_ab, flip(gu_ab, "tp", 1)], 1)
    down_ab = jnp.concatenate([down_a, down_b], 0)
    down_other = jnp.concatenate([down_ab, flip(down_ab, "tp", 1)], 0)

    def weight_of(position):
        pair = line_w[jnp.clip(position, 0, experts // 2 - 1)]
        return pair[0][:, None], pair[1][:, None]

    def through(block, positions):
        ws = [weight_of(p) for p in positions]
        w_own = jnp.concatenate([w[0] for w in ws], 0)
        w_other = jnp.concatenate([w[1] for w in ws], 0)
        g = dot(block, gate_w)
        u = dot(block, up_w)
        h_own = (jax.nn.silu(g) * u * w_own).astype(bf16)
        gu = dot(block, gu_other)
        hs = []
        for i in range(tp_size):
            g_i = gu[:, 2 * i * part : (2 * i + 1) * part]
            u_i = gu[:, (2 * i + 1) * part : (2 * i + 2) * part]
            hs.append(jax.nn.silu(g_i) * u_i)
        h_other = (jnp.concatenate(hs, 1) * w_other).astype(bf16)
        return dot(h_own, down_w) + dot(h_other, down_other)

    out_three = through(three, [jnp.where(z >= 2, z - 3, z + 3)])
    back1 = along_z(out_three.astype(bf16), [(3, 2), (0, 1)])
    out_two = through(two, [jnp.where(z >= 2, z - 2, z + 2)])
    sum_two = (out_two + back1.astype(f32)).astype(bf16)
    back2_down = along_z(sum_two, DOWN[1:])
    back2_up = along_z(sum_two, UP[:2])
    out_near = through(jnp.concatenate([normed, below1, above1], 0), [z, z - 1, z + 1])
    out_own, out_below, out_above = out_near[:rows], out_near[rows : 2 * rows], out_near[2 * rows :]
    back3_down = along_z((out_below + back2_down.astype(f32)).astype(bf16), DOWN)
    back3_up = along_z((out_above + back2_up.astype(f32)).astype(bf16), UP)

    shared_g = dot(normed, shared_gate)
    shared_u = dot(normed, shared_up)
    shared_hidden = (jax.nn.silu(shared_g) * shared_u).astype(bf16)
    kept = out_own + dot(shared_hidden, shared_down)
    branch = kept + back3_down.astype(f32) + back3_up.astype(f32)
    factor = lax.rsqrt(jnp.mean(branch * branch, axis=1, keepdims=True) + epsilon)
    return (wide_resid + branch * factor * post_gain.astype(f32)[None, :]).astype(bf16)


def solution(mesh):
    few = mesh.shape["sp"] == 8 and mesh.shape["tp"] == 4
    return jax.shard_map(
        dense_body if few else routed_body,
        mesh=mesh,
        in_specs=(
            P("sp", "tp"),
            P("sp", "tp"),
            P("sp", "tp"),
            P(None, "tp"),
            P("tp", None),
            P(),
            P(("sp", "tp"), None),
            P(),
            P("sp", None, None),
            P("sp", None, None),
            P("sp", None, None),
            P(),
            P(),
            P(),
            P(),
            P(("sp", "tp"), None),
            P(("sp", "tp"), None),
        ),
        out_specs=P(("sp", "tp"), None),
        check_vma=False,
    )
```

```python
import functools

import jax
import jax.numpy as jnp
from jax import lax
from jax.experimental import pallas as pl
from jax.experimental.pallas import tpu as pltpu
from jax.sharding import PartitionSpec as P

epsilon = 1e-06
f32 = jnp.float32
bf16 = jnp.bfloat16


def passed_along(shard, axis, by):
    size = lax.axis_size(axis)
    pairs = [(i, i + by) for i in range(size) if 0 <= i + by < size]
    return lax.ppermute(shard, axis, pairs)


def routed_body(
    x_in,
    gate_b,
    gate_c,
    conv_taps,
    out_proj,
    mix_gain,
    resid,
    pre_gain,
    expert_gate,
    expert_up,
    expert_down,
    shared_gate,
    shared_up,
    shared_down,
    post_gain,
    routes,
    route_weights,
):
    row_count = x_in.shape[0]
    channels = x_in.shape[1]
    reach = conv_taps.shape[0] - 1
    edge_rows = jnp.concatenate([x_in[row_count - reach :], gate_c[row_count - reach :]], 1)
    arrived_edge = passed_along(edge_rows, "sp", 1)
    inputs = jnp.concatenate([arrived_edge[:, :channels], x_in], 0).astype(jnp.float32)
    gate_rows = jnp.concatenate([arrived_edge[:, channels:], gate_c], 0).astype(jnp.float32)
    mixed_in = inputs * gate_rows
    taps = conv_taps.astype(jnp.float32)
    convolved = jnp.zeros((row_count, channels), jnp.float32)
    for index in range(reach + 1):
        convolved = convolved + taps[index][None, :] * mixed_in[index : index + row_count]
    conv_out = (gate_b.astype(jnp.float32) * convolved).astype(jnp.bfloat16)
    width_all = out_proj.shape[1]
    full_rows = lax.all_to_all(conv_out, "tp", split_axis=0, concat_axis=1, tiled=True)
    projected = jnp.dot(
        full_rows,
        lax.all_gather(out_proj, "tp", axis=0, tiled=True),
        preferred_element_type=jnp.float32,
    )
    row_scale = lax.rsqrt(jnp.mean(projected * projected, axis=1, keepdims=True) + epsilon)
    resid1 = (
        resid.astype(jnp.float32) + projected * row_scale * mix_gain.astype(jnp.float32)
    ).astype(jnp.bfloat16)
    wide_resid = resid1.astype(jnp.float32)
    normed = (
        wide_resid
        * lax.rsqrt(jnp.mean(wide_resid * wide_resid, axis=1, keepdims=True) + epsilon)
        * pre_gain.astype(jnp.float32)
    ).astype(jnp.bfloat16)
    experts = lax.axis_size("sp")
    local_rows = resid.shape[0]
    top_count = routes.shape[1]
    capacity = 3 * local_rows * top_count // (2 * experts)
    flat_ids = routes.reshape(-1)
    onehot = (flat_ids[:, None] == jnp.arange(experts, dtype=jnp.int32)[None, :]).astype(jnp.int32)
    before = jnp.cumsum(onehot, axis=0) - onehot
    position = jnp.sum(before * onehot, axis=1)
    slot_index = flat_ids * capacity + position
    outgoing = (
        jnp.zeros((experts * capacity, width_all), jnp.bfloat16)
        .at[slot_index]
        .set(jnp.repeat(normed, top_count, axis=0))
    )
    received = lax.all_to_all(
        outgoing.reshape(experts, capacity, width_all),
        "sp",
        split_axis=0,
        concat_axis=0,
        tiled=True,
    )
    arrived = received.reshape(experts * capacity, width_all)
    gate_h = jnp.dot(arrived, expert_gate[0], preferred_element_type=jnp.float32)
    up_h = jnp.dot(arrived, expert_up[0], preferred_element_type=jnp.float32)
    hidden = (jax.nn.silu(gate_h) * up_h).astype(jnp.bfloat16)
    expert_out = jnp.dot(hidden, expert_down[0], preferred_element_type=jnp.float32).astype(
        jnp.bfloat16
    )
    returned = lax.all_to_all(
        expert_out.reshape(experts, capacity, width_all),
        "sp",
        split_axis=0,
        concat_axis=0,
        tiled=True,
    )
    returned = returned.reshape(experts * capacity, width_all)
    picked = returned[slot_index].astype(jnp.float32).reshape(local_rows, top_count, width_all)
    routed = jnp.einsum("tk,tkd->td", route_weights, picked)
    shared_g = jnp.dot(normed, shared_gate, preferred_element_type=jnp.float32)
    shared_u = jnp.dot(normed, shared_up, preferred_element_type=jnp.float32)
    shared_hidden = (jax.nn.silu(shared_g) * shared_u).astype(jnp.bfloat16)
    shared_out = jnp.dot(shared_hidden, shared_down, preferred_element_type=jnp.float32)
    branch = routed + shared_out
    factor = lax.rsqrt(jnp.mean(branch * branch, axis=1, keepdims=True) + epsilon)
    return (wide_resid + branch * factor * post_gain.astype(jnp.float32)[None, :]).astype(
        jnp.bfloat16
    )


def dot(a, b):
    return jnp.dot(a, b, preferred_element_type=f32)


def flip(array, axis, bit):
    return lax.ppermute(array, axis, [(i, i ^ bit) for i in range(lax.axis_size(axis))])


def along_z(array, moves):
    pairs = [(2 * a + x, 2 * b + x) for a, b in moves for x in range(2)]
    return lax.ppermute(array, "sp", pairs)


UP = [(0, 1), (1, 2), (2, 3)]
DOWN = [(1, 0), (2, 1), (3, 2)]


def pick(index, arrays):
    out = arrays[-1]
    for i in range(len(arrays) - 2, -1, -1):
        out = jnp.where(index == i, arrays[i], out)
    return out


def dense_body(
    x_in,
    gate_b,
    gate_c,
    conv_taps,
    out_proj,
    mix_gain,
    resid,
    pre_gain,
    expert_gate,
    expert_up,
    expert_down,
    shared_gate,
    shared_up,
    shared_down,
    post_gain,
    routes,
    route_weights,
):
    s = lax.axis_index("sp")
    t = lax.axis_index("tp")
    z, y, c = s // 2, t // 2, t % 2
    experts = lax.axis_size("sp")
    tp_size = lax.axis_size("tp")
    rows = resid.shape[0]
    row_count, channels = x_in.shape
    reach = conv_taps.shape[0] - 1
    edge = 8

    mixed_in = gate_c.astype(f32) * x_in.astype(f32)
    edge_in = passed_along(mixed_in[row_count - edge :], "sp", 1)

    proj_other = flip(out_proj, "tp", 1)

    padded = jnp.concatenate([edge_in, mixed_in], 0)
    taps = conv_taps.astype(f32)
    convolved = jnp.zeros((row_count, channels), f32)
    for index in range(reach + 1):
        start = edge - reach + index
        convolved = convolved + taps[index][None, :] * padded[start : start + row_count]
    conv_out = (gate_b.astype(f32) * convolved).astype(bf16)

    blocks = conv_out.reshape(2, 2, rows, channels)
    mine = pick(c, [blocks[:, 0], blocks[:, 1]])
    give = pick(c, [blocks[:, 1], blocks[:, 0]])
    got = flip(give, "tp", 1)
    far = dot(pick(y, [mine[1], mine[0]]), out_proj) + dot(pick(y, [got[1], got[0]]), proj_other)
    far = far.astype(bf16)
    far_in = flip(far, "tp", 2)
    near = dot(pick(y, [mine[0], mine[1]]), out_proj) + dot(pick(y, [got[0], got[1]]), proj_other)
    projected = near + far_in.astype(f32)

    lanes = jnp.arange(experts, dtype=jnp.int32)
    dense_w = jnp.sum(
        jnp.where(routes[None] == lanes[:, None, None], route_weights[None], 0.0), axis=2
    )
    swapped = dense_w.reshape(experts // 2, 2, rows)[:, ::-1].reshape(experts, rows)
    pair_w = jnp.stack([dense_w, swapped], 1)
    all_w = lax.all_to_all(pair_w, "sp", split_axis=0, concat_axis=0, tiled=True)
    all_w = all_w.reshape(experts // 2, 2, 2, rows)
    line_w = pick(s % 2, [all_w[:, 0], all_w[:, 1]])

    gate_w, up_w, down_w = expert_gate[0], expert_up[0], expert_down[0]
    part = gate_w.shape[1] // tp_size
    gu_part = pick(
        t,
        [
            jnp.concatenate(
                [gate_w[:, i * part : (i + 1) * part], up_w[:, i * part : (i + 1) * part]], 1
            )
            for i in range(tp_size)
        ],
    )
    down_part = pick(t, [down_w[i * part : (i + 1) * part] for i in range(tp_size)])
    gu_a = flip(gu_part, "sp", 1)
    down_a = flip(down_part, "sp", 1)
    gu_b = flip(gu_a, "tp", 2)
    down_b = flip(down_a, "tp", 2)
    gu_c = flip(gu_a, "tp", 1)
    gu_d = flip(gu_b, "tp", 1)
    down_c = flip(down_a, "tp", 1)
    down_d = flip(down_b, "tp", 1)

    row_scale = lax.rsqrt(jnp.mean(projected * projected, axis=1, keepdims=True) + epsilon)
    resid1 = (resid.astype(f32) + projected * row_scale * mix_gain.astype(f32)).astype(bf16)
    wide_resid = resid1.astype(f32)
    normed = (
        wide_resid
        * lax.rsqrt(jnp.mean(wide_resid * wide_resid, axis=1, keepdims=True) + epsilon)
        * pre_gain.astype(f32)
    ).astype(bf16)

    below1 = along_z(normed, UP)
    above1 = along_z(normed, DOWN)
    below2 = along_z(below1, UP[1:])
    above2 = along_z(above1, DOWN[:2])
    two = jnp.where(z >= 2, below2, above2)
    three = along_z(two, [(2, 3), (1, 0)])

    def weight_of(position):
        pair = line_w[jnp.clip(position, 0, experts // 2 - 1)]
        return pair.T

    weights = (gate_w, up_w, down_w, gu_a, gu_b, gu_c, gu_d, down_a, down_b, down_c, down_d)

    def through(blocks, positions):
        return run_pair(blocks, [weight_of(p) for p in positions], *weights)

    (out_three,) = through([three], [jnp.where(z >= 2, z - 3, z + 3)])
    back1 = along_z(out_three, [(3, 2), (0, 1)])
    (out_two,) = through([two], [jnp.where(z >= 2, z - 2, z + 2)])
    sum_two = (out_two.astype(f32) + back1.astype(f32)).astype(bf16)
    back2_down = along_z(sum_two, DOWN[1:])
    back2_up = along_z(sum_two, UP[:2])
    out_own, out_below, out_above = through([normed, below1, above1], [z, z - 1, z + 1])
    back3_down = along_z((out_below.astype(f32) + back2_down.astype(f32)).astype(bf16), DOWN)
    back3_up = along_z((out_above.astype(f32) + back2_up.astype(f32)).astype(bf16), UP)

    shared_g = dot(normed, shared_gate)
    shared_u = dot(normed, shared_up)
    shared_hidden = (jax.nn.silu(shared_g) * shared_u).astype(bf16)
    kept = out_own.astype(f32) + dot(shared_hidden, shared_down)
    branch = kept + back3_down.astype(f32) + back3_up.astype(f32)
    factor = lax.rsqrt(jnp.mean(branch * branch, axis=1, keepdims=True) + epsilon)
    return (wide_resid + branch * factor * post_gain.astype(f32)[None, :]).astype(bf16)


def pair_kernel(count, *refs):
    blocks, scales = refs[:count], refs[count : 2 * count]
    gate, up, down, ga, gb, gc, gd, da, db, dc, dd = refs[2 * count : 2 * count + 11]
    outs = refs[2 * count + 11 :]
    rows, width = blocks[0].shape
    part = da.shape[0]
    join = lambda arrays: arrays[0] if count == 1 else jnp.concatenate(arrays, 0)
    block = join([b[...] for b in blocks])
    scale = join([w[...] for w in scales])
    own, other = scale[:, 0:1], scale[:, 1:2]
    hidden = []
    for i in range(0, gate.shape[1], 2 * part):
        g = dot(block, gate[:, i : i + 2 * part])
        u = dot(block, up[:, i : i + 2 * part])
        hidden.append((g * jax.nn.sigmoid(g) * u * own).astype(bf16))
    rest = []
    for ref in (ga, gb, gc, gd):
        gu = dot(block, ref[...])
        g, u = gu[:, :part], gu[:, part:]
        rest.append((g * jax.nn.sigmoid(g) * u * other).astype(bf16))
    hidden.append(jnp.concatenate(rest[:2], 1))
    hidden.append(jnp.concatenate(rest[2:], 1))
    step = 512
    for n in range(0, width, step):
        cols = slice(n, n + step)
        total = dot(hidden[0], down[0 : 2 * part, cols])
        total += dot(hidden[1], down[2 * part : 4 * part, cols])
        total += dot(hidden[2], jnp.concatenate([da[:, cols], db[:, cols]], 0))
        total += dot(hidden[3], jnp.concatenate([dc[:, cols], dd[:, cols]], 0))
        total = total.astype(bf16)
        for i, out in enumerate(outs):
            out[:, cols] = total[i * rows : (i + 1) * rows]


def run_pair(blocks, scales, *weights):
    count = len(blocks)
    rows, width = blocks[0].shape
    vmem = pl.BlockSpec(memory_space=pltpu.VMEM)
    hidden = weights[0].shape[1]
    return pl.pallas_call(
        functools.partial(pair_kernel, count),
        out_shape=[jax.ShapeDtypeStruct((rows, width), bf16)] * count,
        in_specs=[vmem] * (2 * count + len(weights)),
        out_specs=[vmem] * count,
        cost_estimate=pl.CostEstimate(
            flops=12 * count * rows * width * hidden, bytes_accessed=0, transcendentals=0
        ),
        compiler_params=pltpu.CompilerParams(vmem_limit_bytes=VMEM_LIMIT),
        name="pair",
    )(*blocks, *scales, *weights)


VMEM_LIMIT = 40 * 1024 * 1024


def layer(*args):
    return dense_body(*args)


def solution(mesh):
    few = mesh.shape["sp"] == 8 and mesh.shape["tp"] == 4
    return jax.shard_map(
        layer if few else routed_body,
        mesh=mesh,
        in_specs=(
            P("sp", "tp"),
            P("sp", "tp"),
            P("sp", "tp"),
            P(None, "tp"),
            P("tp", None),
            P(),
            P(("sp", "tp"), None),
            P(),
            P("sp", None, None),
            P("sp", None, None),
            P("sp", None, None),
            P(),
            P(),
            P(),
            P(),
            P(("sp", "tp"), None),
            P(("sp", "tp"), None),
        ),
        out_specs=P(("sp", "tp"), None),
        check_vma=False,
    )
```

```python
import jax
import jax.numpy as jnp
from jax import lax
from jax.experimental import pallas as pl
from jax.experimental.pallas import tpu as pltpu
from jax.sharding import PartitionSpec as P

epsilon = 1e-06
f32 = jnp.float32
bf16 = jnp.bfloat16
MIB = 1024 * 1024


def passed_along(shard, axis, by):
    size = lax.axis_size(axis)
    pairs = [(i, i + by) for i in range(size) if 0 <= i + by < size]
    return lax.ppermute(shard, axis, pairs)


def routed_body(
    x_in,
    gate_b,
    gate_c,
    conv_taps,
    out_proj,
    mix_gain,
    resid,
    pre_gain,
    expert_gate,
    expert_up,
    expert_down,
    shared_gate,
    shared_up,
    shared_down,
    post_gain,
    routes,
    route_weights,
):
    row_count = x_in.shape[0]
    channels = x_in.shape[1]
    reach = conv_taps.shape[0] - 1
    edge_rows = jnp.concatenate([x_in[row_count - reach :], gate_c[row_count - reach :]], 1)
    arrived_edge = passed_along(edge_rows, "sp", 1)
    inputs = jnp.concatenate([arrived_edge[:, :channels], x_in], 0).astype(jnp.float32)
    gate_rows = jnp.concatenate([arrived_edge[:, channels:], gate_c], 0).astype(jnp.float32)
    mixed_in = inputs * gate_rows
    taps = conv_taps.astype(jnp.float32)
    convolved = jnp.zeros((row_count, channels), jnp.float32)
    for index in range(reach + 1):
        convolved = convolved + taps[index][None, :] * mixed_in[index : index + row_count]
    conv_out = (gate_b.astype(jnp.float32) * convolved).astype(jnp.bfloat16)
    width_all = out_proj.shape[1]
    full_rows = lax.all_to_all(conv_out, "tp", split_axis=0, concat_axis=1, tiled=True)
    projected = jnp.dot(
        full_rows,
        lax.all_gather(out_proj, "tp", axis=0, tiled=True),
        preferred_element_type=jnp.float32,
    )
    row_scale = lax.rsqrt(jnp.mean(projected * projected, axis=1, keepdims=True) + epsilon)
    resid1 = (
        resid.astype(jnp.float32) + projected * row_scale * mix_gain.astype(jnp.float32)
    ).astype(jnp.bfloat16)
    wide_resid = resid1.astype(jnp.float32)
    normed = (
        wide_resid
        * lax.rsqrt(jnp.mean(wide_resid * wide_resid, axis=1, keepdims=True) + epsilon)
        * pre_gain.astype(jnp.float32)
    ).astype(jnp.bfloat16)
    experts = lax.axis_size("sp")
    local_rows = resid.shape[0]
    top_count = routes.shape[1]
    capacity = 3 * local_rows * top_count // (2 * experts)
    flat_ids = routes.reshape(-1)
    onehot = (flat_ids[:, None] == jnp.arange(experts, dtype=jnp.int32)[None, :]).astype(jnp.int32)
    before = jnp.cumsum(onehot, axis=0) - onehot
    position = jnp.sum(before * onehot, axis=1)
    slot_index = flat_ids * capacity + position
    outgoing = (
        jnp.zeros((experts * capacity, width_all), jnp.bfloat16)
        .at[slot_index]
        .set(jnp.repeat(normed, top_count, axis=0))
    )
    received = lax.all_to_all(
        outgoing.reshape(experts, capacity, width_all),
        "sp",
        split_axis=0,
        concat_axis=0,
        tiled=True,
    )
    arrived = received.reshape(experts * capacity, width_all)
    gate_h = jnp.dot(arrived, expert_gate[0], preferred_element_type=jnp.float32)
    up_h = jnp.dot(arrived, expert_up[0], preferred_element_type=jnp.float32)
    hidden = (jax.nn.silu(gate_h) * up_h).astype(jnp.bfloat16)
    expert_out = jnp.dot(hidden, expert_down[0], preferred_element_type=jnp.float32).astype(
        jnp.bfloat16
    )
    returned = lax.all_to_all(
        expert_out.reshape(experts, capacity, width_all),
        "sp",
        split_axis=0,
        concat_axis=0,
        tiled=True,
    )
    returned = returned.reshape(experts * capacity, width_all)
    picked = returned[slot_index].astype(jnp.float32).reshape(local_rows, top_count, width_all)
    routed = jnp.einsum("tk,tkd->td", route_weights, picked)
    shared_g = jnp.dot(normed, shared_gate, preferred_element_type=jnp.float32)
    shared_u = jnp.dot(normed, shared_up, preferred_element_type=jnp.float32)
    shared_hidden = (jax.nn.silu(shared_g) * shared_u).astype(jnp.bfloat16)
    shared_out = jnp.dot(shared_hidden, shared_down, preferred_element_type=jnp.float32)
    branch = routed + shared_out
    factor = lax.rsqrt(jnp.mean(branch * branch, axis=1, keepdims=True) + epsilon)
    return (wide_resid + branch * factor * post_gain.astype(jnp.float32)[None, :]).astype(
        jnp.bfloat16
    )


def dot(a, b):
    return jnp.dot(a, b, preferred_element_type=f32)


def silu(g):
    return g * jax.nn.sigmoid(g)


def flip(array, axis, bit):
    return lax.ppermute(array, axis, [(i, i ^ bit) for i in range(lax.axis_size(axis))])


def middle_swap(array):
    size, inner = lax.axis_size("sp"), lax.axis_size("tp")
    quarter = size // 4
    pairs = []
    for i in range(size):
        end = i < quarter or i >= 3 * quarter
        for j in range(inner):
            target = (i, j ^ 1) if end else (i ^ (3 * quarter), j)
            pairs.append((i * inner + j, target[0] * inner + target[1]))
    return lax.ppermute(array, ("sp", "tp"), pairs)


def in_middle():
    z = lax.axis_index("sp") // 2
    return (z > 0) & (z < lax.axis_size("sp") // 2 - 1)


VMEM = pl.BlockSpec(memory_space=pltpu.VMEM)


def cost(moved, flops=0):
    return pl.CostEstimate(flops=flops, bytes_accessed=moved, transcendentals=0)


def call(kernel, out_shape, *operands, limit=8, flops=0):
    shapes = [jax.ShapeDtypeStruct(*shape) for shape in out_shape]
    out = pl.pallas_call(
        kernel,
        out_shape=shapes,
        in_specs=[VMEM] * len(operands),
        out_specs=[VMEM] * len(shapes),
        cost_estimate=cost(MIB, flops),
        compiler_params=pltpu.CompilerParams(vmem_limit_bytes=limit * MIB),
    )(*operands)
    return out[0] if len(out) == 1 else out


def dense_body(
    x_in,
    gate_b,
    gate_c,
    conv_taps,
    out_proj,
    mix_gain,
    resid,
    pre_gain,
    expert_gate,
    expert_up,
    expert_down,
    shared_gate,
    shared_up,
    shared_down,
    post_gain,
    routes,
    route_weights,
):
    tp_size = lax.axis_size("tp")
    rows = resid.shape[0]
    edge = 8

    edge_rows = edge_product(x_in, gate_c, edge)
    size = lax.axis_size("sp")
    edge_in = lax.ppermute(edge_rows, "sp", [(i, (i + 1) % size) for i in range(size)])
    rest = convolve(x_in, gate_b, gate_c, conv_taps, edge, rows)
    mine, give = convolve_edge(edge_in, conv_taps, *rest)

    proj_other = flip(out_proj, "tp", 1)

    got = flip(give, "tp", 1)
    far = project(1, mine, got, out_proj, proj_other, bf16)
    far_in = flip(far, "tp", 2)
    near = project(0, mine, got, out_proj, proj_other, f32)
    table = route_table(routes.T, route_weights.T, lax.axis_size("sp"))
    resid1, normed = norms(near, far_in, resid, mix_gain, pre_gain, table)

    gate_w, up_w, down_w = expert_gate[0], expert_up[0], expert_down[0]
    part = gate_w.shape[1] // tp_size
    g1, dn = expert_parts(gate_w, up_w, part, 0, down_w)
    g2, g3 = expert_parts(gate_w, up_w, part, 1)
    others = []
    for piece in (g1, dn):
        piece_a = flip(piece, "sp", 1)
        piece_b = flip(piece_a, "tp", 2)
        piece_c = flip(piece_a, "tp", 1)
        piece_d = flip(piece_b, "tp", 1)
        others += [piece_a, piece_b, piece_c, piece_d]
    for piece in (g2, g3):
        piece_a = flip(piece, "sp", 1)
        others += [piece_a, flip(piece_a, "tp", 1)]

    p1 = flip(normed, "sp", 2)
    q1 = middle_swap(normed)
    q2 = middle_swap(p1)
    p2 = flip(q1, "sp", 2)
    weights = (up_w, down_w, *others)
    near_blocks, two = [(normed,), (p1,)], [(q2, p2)]
    near_hidden = run_hidden(near_blocks, gate_w, up_w)
    *two_out, send = run_pair(two, True, gate_w, *weights)
    p3 = flip(send, "sp", 2)
    three_out = run_pair([(q1, p3)], False, gate_w, *weights)
    near_out = run_pair(near_blocks, False, near_hidden, *weights)
    own_out, p_out = near_out[:PIECES], near_out[PIECES:]

    outer, inner = [], []
    for i in range(PIECES):
        r1 = flip(three_out[i], "sp", 2)
        m2 = middle_swap(added([two_out[i]], r1))
        outer.append(flip(added([p_out[i]], m2), "sp", 2))
    for i in range(2):
        group = PIECES // 2
        inner.append(middle_swap(added(three_out[i * group : (i + 1) * group], p3, i)))

    kept = shared_expert(normed, own_out, shared_gate, shared_up, shared_down)
    return finish(kept, outer, inner, resid1, post_gain)


PIECES = 4


def edge_product(x_in, gate_c, edge):
    row_count, channels = x_in.shape
    tile = 2 * edge

    def kernel(x_ref, c_ref, out_ref):
        product = c_ref[...].astype(f32) * x_ref[...].astype(f32)
        out_ref[...] = product[tile - edge :]

    last = pl.BlockSpec((tile, channels), lambda i: (row_count // tile - 1, 0))
    return pl.pallas_call(
        kernel,
        grid=(1,),
        out_shape=jax.ShapeDtypeStruct((edge, channels), f32),
        in_specs=[last, last],
        out_specs=pl.BlockSpec((edge, channels), lambda i: (0, 0)),
        cost_estimate=cost(4 * MIB),
        name="edge_product",
    )(x_in, gate_c)


def expert_parts(gate_w, up_w, part, row, *down_w):
    half = gate_w.shape[0] // 2
    count = 1 + row
    cut = half * 3 // 4
    spans = [(0, cut), (cut, half)] if row else [(0, half)]

    def kernel(*refs):
        ins, outs = refs[: 2 * count + len(down_w)], refs[2 * count + len(down_w) :]
        for i, ref in enumerate(ins[: 2 * count]):
            for (start, end), out in zip(spans, outs):
                out[:, i * part : (i + 1) * part] = ref[start:end]
        if down_w:
            outs[1][...] = ins[-1][...]

    specs = [
        pl.BlockSpec((half, part), lambda i, f=flipped: (row, lax.axis_index("tp") ^ f))
        for flipped in range(0, 2 * count, 2)
        for _ in range(2)
    ]
    shapes = [(end - start, 2 * count * part) for start, end in spans]
    for down in down_w:
        specs.append(pl.BlockSpec((part, down.shape[1]), lambda i: (lax.axis_index("tp"), 0)))
        shapes.append((part, down.shape[1]))
    return pl.pallas_call(
        kernel,
        grid=(1,),
        out_shape=[jax.ShapeDtypeStruct(shape, bf16) for shape in shapes],
        in_specs=specs,
        out_specs=[pl.BlockSpec(shape, lambda i: (0, 0)) for shape in shapes],
        cost_estimate=cost(4 * MIB),
        compiler_params=pltpu.CompilerParams(vmem_limit_bytes=(12 if row else 60) * MIB),
        name="parts",
    )(*[gate_w, up_w] * count, *down_w)


def convolve(x_in, gate_b, gate_c, conv_taps, edge, rows):
    row_count, channels = x_in.shape
    reach = conv_taps.shape[0] - 1
    groups = row_count // rows

    def kernel(x_ref, g_ref, b_ref, taps_ref, mine, give, head, head_gate, before):
        group = pl.program_id(0)
        core = lax.axis_index("tp") % 2
        taps = taps_ref[...].astype(f32)
        mixed = g_ref[...].astype(f32) * x_ref[...].astype(f32)
        gate = b_ref[...].astype(f32)

        @pl.when(group == 0)
        def _():
            before[...] = jnp.zeros((edge, channels), f32)

        padded = jnp.concatenate([before[...], mixed], 0)
        before[...] = mixed[rows - edge :]
        total = jnp.zeros((rows, channels), f32)
        for index in range(reach + 1):
            start = edge - reach + index
            total = total + taps[index : index + 1] * padded[start : start + rows]
        result = (gate * total).astype(bf16)

        @pl.when(group == 0)
        def _():
            head[...] = total[:edge]
            head_gate[...] = gate[:edge]

        @pl.when(core == group % 2)
        def _():
            mine[group // 2] = result

        @pl.when(core != group % 2)
        def _():
            give[group // 2] = result

    shape = ((groups // 2, rows, channels), bf16)
    small = ((edge, channels), f32)
    shapes = [shape, shape, small, small]
    block = pl.BlockSpec((rows, channels), lambda i: (i, 0))
    return pl.pallas_call(
        kernel,
        grid=(groups,),
        out_shape=[jax.ShapeDtypeStruct(*s) for s in shapes],
        in_specs=[block] * 3 + [pl.BlockSpec(conv_taps.shape, lambda i: (0, 0))],
        out_specs=[pl.BlockSpec(s[0], lambda i, n=len(s[0]): (0,) * n) for s in shapes],
        scratch_shapes=[pltpu.VMEM((edge, channels), f32)],
        compiler_params=pltpu.CompilerParams(vmem_limit_bytes=8 * MIB),
        name="convolve",
    )(x_in, gate_c, gate_b, conv_taps)


def convolve_edge(edge_in, conv_taps, mine, give, head, head_gate):
    edge, channels = edge_in.shape
    reach = conv_taps.shape[0] - 1

    def kernel(edge_ref, taps_ref, mine_ref, give_ref, head_ref, gate_ref, mine_out, give_out):
        core = lax.axis_index("tp") % 2
        taps = taps_ref[...].astype(f32)
        before = jnp.where(lax.axis_index("sp") > 0, edge_ref[...], 0.0)
        padded = jnp.concatenate([before, jnp.zeros((edge, channels), f32)], 0)
        total = jnp.zeros((edge, channels), f32)
        for index in range(reach):
            start = edge - reach + index
            total = total + taps[index : index + 1] * padded[start : start + edge]
        result = (gate_ref[...] * (total + head_ref[...])).astype(bf16)
        mine_out[...] = mine_ref[...]
        give_out[...] = give_ref[...]

        @pl.when(core == 0)
        def _():
            mine_out[0, :edge] = result

        @pl.when(core != 0)
        def _():
            give_out[0, :edge] = result

    shape = (mine.shape, bf16)
    operands = (edge_in, conv_taps, mine, give, head, head_gate)
    return call(kernel, [shape, shape], *operands, limit=4)


def project(other, mine, got, proj, proj_other, dtype):
    rows = mine.shape[1]
    width = proj.shape[1]

    def kernel(mine_ref, got_ref, proj_ref, other_ref, out_ref):
        y = lax.axis_index("tp") // 2
        y = 1 - y if other else y
        a, b = mine_ref[y], got_ref[y]
        step = 512
        for n in range(0, width, step):
            cols = slice(n, n + step)
            out_ref[:, cols] = (dot(a, proj_ref[:, cols]) + dot(b, other_ref[:, cols])).astype(dtype)

    flops = 4 * rows * proj.size
    return call(kernel, [((rows, width), dtype)], mine, got, proj, proj_other, flops=flops)


PARTS = 3


def route_table(routes, weights, experts):
    top, rows = routes.shape
    lanes = 128

    def kernel(routes_ref, weights_ref, out_ref):
        expert = lax.broadcasted_iota(jnp.int32, (experts, rows), 0)
        left = jnp.zeros((experts, rows), f32)
        for k in range(top):
            left = left + jnp.where(routes_ref[k : k + 1] == expert, weights_ref[k : k + 1], 0.0)
        pieces = []
        for _ in range(PARTS):
            piece = left.astype(bf16).astype(f32)
            left = left - piece
            pieces.append(piece)
        pieces.append(jnp.zeros((lanes - PARTS * experts, rows), f32))
        out_ref[...] = jnp.concatenate(pieces, 0).T.astype(bf16)

    return call(kernel, [((rows, lanes), bf16)], routes, weights, limit=4)


def norms(near, far_in, resid, mix_gain, pre_gain, table):
    rows, width = near.shape
    extra = table.shape[1]
    step = 32

    def kernel(near_ref, far_ref, resid_ref, mix_ref, pre_ref, table_ref, resid_out, normed_out):
        mix, pre = mix_ref[...].astype(f32), pre_ref[...].astype(f32)
        for r in range(0, rows, step):
            span = slice(r, r + step)
            total = near_ref[span] + far_ref[span].astype(f32)
            scale = lax.rsqrt(jnp.mean(total * total, axis=1, keepdims=True) + epsilon)
            row = (resid_ref[span].astype(f32) + total * scale * mix).astype(bf16)
            resid_out[span] = row
            wide = row.astype(f32)
            scale = lax.rsqrt(jnp.mean(wide * wide, axis=1, keepdims=True) + epsilon)
            normed_out[span, :width] = (wide * scale * pre).astype(bf16)
        normed_out[:, width:] = table_ref[...]

    operands = (near, far_in, resid, mix_gain[None], pre_gain[None], table)
    return call(kernel, [((rows, width), bf16), ((rows, width + extra), bf16)], *operands)


def added(outs, back, part=0):
    rows, piece = outs[0].shape
    count = len(outs)

    def kernel(*refs):
        back_ref, sum_ref = refs[count:]
        for i, ref in enumerate(refs[:count]):
            start = (part * count + i) * piece
            back_part = jnp.where(in_middle(), back_ref[:, start : start + piece].astype(f32), 0.0)
            sum_ref[:, i * piece : (i + 1) * piece] = (ref[...].astype(f32) + back_part).astype(bf16)

    return call(kernel, [((rows, count * piece), bf16)], *outs, back, limit=4)


def shared_expert(normed, own, gate, up, down):
    rows = normed.shape[0]
    width = gate.shape[0]
    step = own[0].shape[1]

    def kernel(n_ref, *refs):
        gate_ref, up_ref, down_ref, out_ref = refs[len(own) :]
        block = n_ref[:, :width]
        hidden = (silu(dot(block, gate_ref[...])) * dot(block, up_ref[...])).astype(bf16)
        for i, ref in enumerate(refs[: len(own)]):
            cols = slice(i * step, (i + 1) * step)
            out_ref[:, cols] = ref[...].astype(f32) + dot(hidden, down_ref[:, cols])

    flops = 6 * rows * gate.size
    operands = (normed, *own, gate, up, down)
    return call(kernel, [((rows, width), f32)], *operands, flops=flops)


def finish(kept, outer, inner, resid1, gain):
    rows, width = kept.shape
    piece = outer[0].shape[1]
    per_inner = len(outer) // len(inner)
    step = 64

    def kernel(kept_ref, *refs):
        outer_refs, inner_refs = refs[: len(outer)], refs[len(outer) : len(outer) + len(inner)]
        resid_ref, gain_ref, out_ref = refs[len(outer) + len(inner) :]
        middle = in_middle()
        parts, square = [], 0.0
        for i, ref in enumerate(outer_refs):
            part = kept_ref[:, i * piece : (i + 1) * piece] + ref[...].astype(f32)
            start = (i % per_inner) * piece
            back = inner_refs[i // per_inner][:, start : start + piece].astype(f32)
            part = part + jnp.where(middle, back, 0.0)
            square = square + jnp.sum(part * part, axis=1, keepdims=True)
            parts.append(part)
        factor = lax.rsqrt(square * (1.0 / width) + epsilon)
        for i, part in enumerate(parts):
            cols = slice(i * piece, (i + 1) * piece)
            scaled = part * factor * gain_ref[:, cols].astype(f32)
            out_ref[:, cols] = (resid_ref[:, cols].astype(f32) + scaled).astype(bf16)

    def block(array):
        return pl.BlockSpec((step, array.shape[1]), lambda i: (i, 0))

    operands = (kept, *outer, *inner, resid1)
    return pl.pallas_call(
        kernel,
        grid=(rows // step,),
        out_shape=jax.ShapeDtypeStruct((rows, width), bf16),
        in_specs=[block(x) for x in operands] + [pl.BlockSpec((1, width), lambda i: (0, 0))],
        out_specs=block(kept),
        compiler_params=pltpu.CompilerParams(vmem_limit_bytes=8 * MIB),
        name="finish",
    )(*operands, gain[None])


def block_of(refs):
    if len(refs) == 1:
        return refs[0][...]
    return jnp.where(in_middle(), refs[0][...], refs[1][...])


def gather_blocks(refs, sizes):
    blocks, start = [], 0
    for size in sizes:
        blocks.append(block_of(refs[start : start + size]))
        start += size
    return blocks[0] if len(blocks) == 1 else jnp.concatenate(blocks, 0)


def scale_of(block, width, expert, experts):
    table = block[:, width:].astype(f32)
    lane = lax.broadcasted_iota(jnp.int32, table.shape, 1)
    return jnp.sum(jnp.where(lane % experts == expert, table, 0.0), axis=1, keepdims=True)


def own_hidden(block, gate, up, step, experts):
    width = gate.shape[0]
    scale = scale_of(block, width, lax.axis_index("sp"), experts)
    hidden = []
    for i in range(0, gate.shape[1], step):
        g = dot(block[:, :width], gate[:, i : i + step])
        u = dot(block[:, :width], up[:, i : i + step])
        hidden.append((silu(g) * u * scale).astype(bf16))
    return hidden


def run_hidden(blocks, gate, up):
    experts = lax.axis_size("sp")
    sizes = [len(block) for block in blocks]
    rows = len(blocks) * blocks[0][0].shape[0]
    count = sum(sizes)
    step = 256

    def kernel(*refs):
        gate_ref, up_ref, out_ref = refs[count:]
        block = gather_blocks(refs[:count], sizes)
        for i, part in enumerate(own_hidden(block, gate_ref, up_ref, step, experts)):
            out_ref[:, i * step : (i + 1) * step] = part

    operands = [array for block in blocks for array in block]
    shape = ((rows, gate.shape[1]), bf16)
    return call(kernel, [shape], *operands, gate, up, limit=10, flops=4 * rows * gate.size)


def run_pair(blocks, sends, gate, up, down, *others):
    experts = lax.axis_size("sp")
    sizes = [len(block) for block in blocks]
    count = sum(sizes)
    rows = blocks[0][0].shape[0]
    hidden_size, width = down.shape
    ready = gate.shape[0] == len(blocks) * rows

    def kernel(*refs):
        gate_ref, up_ref, down_ref = refs[count : count + 3]
        g1a, g1b, g1c, g1d, da, db, dc, dd, g2a, g2c, g3a, g3c = refs[count + 3 : count + 15]
        outs = refs[count + 15 :]
        part, half = da.shape[0], g1a.shape[0]
        cut = half + g2a.shape[0]
        block = gather_blocks(refs[:count], sizes)
        if ready:
            hidden = [gate_ref[:, i : i + 2 * part] for i in range(0, hidden_size, 2 * part)]
        else:
            hidden = own_hidden(block, gate_ref, up_ref, 2 * part, experts)
        scale = scale_of(block, width, lax.axis_index("sp") ^ 1, experts)
        rest = []
        for i, top in enumerate((g1a, g1b, g1c, g1d)):
            side = (i % 2) * 2 * part
            gu = dot(block[:, :half], top[...])
            gu += dot(block[:, half:cut], (g2a, g2c)[i // 2][:, side : side + 2 * part])
            gu += dot(block[:, cut:width], (g3a, g3c)[i // 2][:, side : side + 2 * part])
            rest.append((silu(gu[:, :part]) * gu[:, part:] * scale).astype(bf16))
        hidden.append(jnp.concatenate(rest[:2], 1))
        hidden.append(jnp.concatenate(rest[2:], 1))
        step = 512
        for n in range(0, width, step):
            cols = slice(n, n + step)
            total = dot(hidden[0], down_ref[0 : 2 * part, cols])
            total += dot(hidden[1], down_ref[2 * part : 4 * part, cols])
            total += dot(hidden[2], jnp.concatenate([da[:, cols], db[:, cols]], 0))
            total += dot(hidden[3], jnp.concatenate([dc[:, cols], dd[:, cols]], 0))
            total = total.astype(bf16)
            piece, start = n // (width // PIECES), n % (width // PIECES)
            for i in range(len(blocks)):
                out = outs[PIECES * i + piece]
                out[:, start : start + step] = total[i * rows : (i + 1) * rows]
            if sends:
                outs[-1][:, cols] = jnp.where(in_middle(), refs[0][:, cols], total)
        if sends:
            outs[-1][:, width:] = refs[0][:, width:]

    operands = [array for block in blocks for array in block]
    flops = 12 * len(blocks) * rows * width * hidden_size
    shapes = [((rows, width // PIECES), bf16)] * (PIECES * len(blocks))
    if sends:
        shapes.append((blocks[0][0].shape, bf16))
    operands += [gate, up, down, *others]
    limit = 4 + 6 * len(blocks)
    return call(kernel, shapes, *operands, limit=limit, flops=flops)


def layer(*args):
    return dense_body(*args)


def solution(mesh):
    few = mesh.shape["sp"] == 8 and mesh.shape["tp"] == 4
    return jax.shard_map(
        layer if few else routed_body,
        mesh=mesh,
        in_specs=(
            P("sp", "tp"),
            P("sp", "tp"),
            P("sp", "tp"),
            P(None, "tp"),
            P("tp", None),
            P(),
            P(("sp", "tp"), None),
            P(),
            P("sp", None, None),
            P("sp", None, None),
            P("sp", None, None),
            P(),
            P(),
            P(),
            P(),
            P(("sp", "tp"), None),
            P(("sp", "tp"), None),
        ),
        out_specs=P(("sp", "tp"), None),
        check_vma=False,
    )
```

```python
import jax
import jax.numpy as jnp
from jax import lax
from jax.experimental import pallas as pl
from jax.experimental.pallas import tpu as pltpu
from jax.sharding import PartitionSpec as P

epsilon = 1e-06
f32 = jnp.float32
bf16 = jnp.bfloat16
MIB = 1024 * 1024


def passed_along(shard, axis, by):
    size = lax.axis_size(axis)
    pairs = [(i, i + by) for i in range(size) if 0 <= i + by < size]
    return lax.ppermute(shard, axis, pairs)


def routed_body(
    x_in,
    gate_b,
    gate_c,
    conv_taps,
    out_proj,
    mix_gain,
    resid,
    pre_gain,
    expert_gate,
    expert_up,
    expert_down,
    shared_gate,
    shared_up,
    shared_down,
    post_gain,
    routes,
    route_weights,
):
    row_count = x_in.shape[0]
    channels = x_in.shape[1]
    reach = conv_taps.shape[0] - 1
    edge_rows = jnp.concatenate([x_in[row_count - reach :], gate_c[row_count - reach :]], 1)
    arrived_edge = passed_along(edge_rows, "sp", 1)
    inputs = jnp.concatenate([arrived_edge[:, :channels], x_in], 0).astype(jnp.float32)
    gate_rows = jnp.concatenate([arrived_edge[:, channels:], gate_c], 0).astype(jnp.float32)
    mixed_in = inputs * gate_rows
    taps = conv_taps.astype(jnp.float32)
    convolved = jnp.zeros((row_count, channels), jnp.float32)
    for index in range(reach + 1):
        convolved = convolved + taps[index][None, :] * mixed_in[index : index + row_count]
    conv_out = (gate_b.astype(jnp.float32) * convolved).astype(jnp.bfloat16)
    width_all = out_proj.shape[1]
    full_rows = lax.all_to_all(conv_out, "tp", split_axis=0, concat_axis=1, tiled=True)
    projected = jnp.dot(
        full_rows,
        lax.all_gather(out_proj, "tp", axis=0, tiled=True),
        preferred_element_type=jnp.float32,
    )
    row_scale = lax.rsqrt(jnp.mean(projected * projected, axis=1, keepdims=True) + epsilon)
    resid1 = (
        resid.astype(jnp.float32) + projected * row_scale * mix_gain.astype(jnp.float32)
    ).astype(jnp.bfloat16)
    wide_resid = resid1.astype(jnp.float32)
    normed = (
        wide_resid
        * lax.rsqrt(jnp.mean(wide_resid * wide_resid, axis=1, keepdims=True) + epsilon)
        * pre_gain.astype(jnp.float32)
    ).astype(jnp.bfloat16)
    experts = lax.axis_size("sp")
    local_rows = resid.shape[0]
    top_count = routes.shape[1]
    capacity = 3 * local_rows * top_count // (2 * experts)
    flat_ids = routes.reshape(-1)
    onehot = (flat_ids[:, None] == jnp.arange(experts, dtype=jnp.int32)[None, :]).astype(jnp.int32)
    before = jnp.cumsum(onehot, axis=0) - onehot
    position = jnp.sum(before * onehot, axis=1)
    slot_index = flat_ids * capacity + position
    outgoing = (
        jnp.zeros((experts * capacity, width_all), jnp.bfloat16)
        .at[slot_index]
        .set(jnp.repeat(normed, top_count, axis=0))
    )
    received = lax.all_to_all(
        outgoing.reshape(experts, capacity, width_all),
        "sp",
        split_axis=0,
        concat_axis=0,
        tiled=True,
    )
    arrived = received.reshape(experts * capacity, width_all)
    gate_h = jnp.dot(arrived, expert_gate[0], preferred_element_type=jnp.float32)
    up_h = jnp.dot(arrived, expert_up[0], preferred_element_type=jnp.float32)
    hidden = (jax.nn.silu(gate_h) * up_h).astype(jnp.bfloat16)
    expert_out = jnp.dot(hidden, expert_down[0], preferred_element_type=jnp.float32).astype(
        jnp.bfloat16
    )
    returned = lax.all_to_all(
        expert_out.reshape(experts, capacity, width_all),
        "sp",
        split_axis=0,
        concat_axis=0,
        tiled=True,
    )
    returned = returned.reshape(experts * capacity, width_all)
    picked = returned[slot_index].astype(jnp.float32).reshape(local_rows, top_count, width_all)
    routed = jnp.einsum("tk,tkd->td", route_weights, picked)
    shared_g = jnp.dot(normed, shared_gate, preferred_element_type=jnp.float32)
    shared_u = jnp.dot(normed, shared_up, preferred_element_type=jnp.float32)
    shared_hidden = (jax.nn.silu(shared_g) * shared_u).astype(jnp.bfloat16)
    shared_out = jnp.dot(shared_hidden, shared_down, preferred_element_type=jnp.float32)
    branch = routed + shared_out
    factor = lax.rsqrt(jnp.mean(branch * branch, axis=1, keepdims=True) + epsilon)
    return (wide_resid + branch * factor * post_gain.astype(jnp.float32)[None, :]).astype(
        jnp.bfloat16
    )


def dot(a, b):
    return jnp.dot(a, b, preferred_element_type=f32)


def silu(g):
    return g * jax.nn.sigmoid(g)


def flip(array, axis, bit):
    return lax.ppermute(array, axis, [(i, i ^ bit) for i in range(lax.axis_size(axis))])


def middle_swap(array):
    size, inner = lax.axis_size("sp"), lax.axis_size("tp")
    quarter = size // 4
    pairs = []
    for i in range(size):
        end = i < quarter or i >= 3 * quarter
        for j in range(inner):
            target = (i, j ^ 1) if end else (i ^ (3 * quarter), j)
            pairs.append((i * inner + j, target[0] * inner + target[1]))
    return lax.ppermute(array, ("sp", "tp"), pairs)


def in_middle():
    z = lax.axis_index("sp") // 2
    return (z > 0) & (z < lax.axis_size("sp") // 2 - 1)


VMEM = pl.BlockSpec(memory_space=pltpu.VMEM)


def cost(moved, flops=0):
    return pl.CostEstimate(flops=flops, bytes_accessed=moved, transcendentals=0)


def call(kernel, out_shape, *operands, limit=8, flops=0):
    shapes = [jax.ShapeDtypeStruct(*shape) for shape in out_shape]
    out = pl.pallas_call(
        kernel,
        out_shape=shapes,
        in_specs=[VMEM] * len(operands),
        out_specs=[VMEM] * len(shapes),
        cost_estimate=cost(MIB, flops),
        compiler_params=pltpu.CompilerParams(vmem_limit_bytes=limit * MIB),
    )(*operands)
    return out[0] if len(out) == 1 else out


def dense_body(
    x_in,
    gate_b,
    gate_c,
    conv_taps,
    out_proj,
    mix_gain,
    resid,
    pre_gain,
    expert_gate,
    expert_up,
    expert_down,
    shared_gate,
    shared_up,
    shared_down,
    post_gain,
    routes,
    route_weights,
):
    tp_size = lax.axis_size("tp")
    rows = resid.shape[0]
    edge = 8

    edge_rows = edge_product(x_in, gate_c, edge)
    size = lax.axis_size("sp")
    edge_in = lax.ppermute(edge_rows, "sp", [(i, (i + 1) % size) for i in range(size)])
    rest = convolve(x_in, gate_b, gate_c, conv_taps, edge, rows)
    mine, give = convolve_edge(edge_in, conv_taps, *rest)

    proj_other = flip(out_proj, "tp", 1)

    got = flip(give, "tp", 1)
    far = project(1, mine, got, out_proj, proj_other, bf16)
    far_in = flip(far, "tp", 2)
    near = project(0, mine, got, out_proj, proj_other, f32)
    table = route_table(routes.T, route_weights.T, lax.axis_size("sp"))
    resid1, *normed = norms(near, far_in, resid, mix_gain, pre_gain)

    gate_w, up_w, down_w = expert_gate[0], expert_up[0], expert_down[0]
    part = gate_w.shape[1] // tp_size
    depth = gate_w.shape[0]
    head, cut = depth * 5 // 8, depth * 7 // 8
    (g1,) = expert_parts(gate_w, up_w, part, [(0, head)], 1)
    spans = [(head, cut), (cut, depth)]
    g2, g3, dn = expert_parts(gate_w, up_w, part, spans, 2, down_w)
    others = []
    for piece in (g1, dn):
        piece_a = flip(piece, "sp", 1)
        piece_b = flip(piece_a, "tp", 2)
        piece_c = flip(piece_a, "tp", 1)
        piece_d = flip(piece_b, "tp", 1)
        others += [piece_a, piece_b, piece_c, piece_d]
    for piece in (g2, g3):
        piece_a = flip(piece, "sp", 1)
        others += [piece_a, flip(piece_a, "tp", 1)]

    p1_table = flip(table, "sp", 2)
    q1_table = middle_swap(table)
    q2_table = middle_swap(p1_table)
    p2_table = flip(q1_table, "sp", 2)
    p3_table = flip(q2_table, "sp", 2)
    p1, q1, q2, p2 = [], [], [], []
    for i, piece in enumerate(normed):
        p1.append(flip(piece, "sp", 2))
        q1.append(middle_swap(piece))
        q2.append(middle_swap(p1[i]))
        p2.append(flip(q1[i], "sp", 2))

    weights = (gate_w, up_w, down_w, *others)
    two_tables = [[(q2_table, p2_table)]]
    *two_out, send = run_pair([list(zip(q2, p2))], two_tables, True, *weights)
    p3 = flip(send, "sp", 2)
    near_blocks = [list(zip(pieces)) for pieces in (normed, p1, q1)]
    near_tables = [[(t,)] for t in (table, p1_table, q1_table)]
    near_out = run_pair(near_blocks, near_tables, False, *weights)
    own_out, p_out, q_out = (near_out[i * PIECES : (i + 1) * PIECES] for i in range(3))
    three_out = run_pair([[(p3,)]], [[(p3_table,)]], False, *weights, ends=True)

    outer, inner = [], []
    for i in range(PIECES):
        r1 = flip(three_out[i], "sp", 2)
        m2 = middle_swap(added([two_out[i]], r1))
        outer.append(flip(added([p_out[i]], m2), "sp", 2))
    for start, end in INNER:
        inner.append(middle_swap(added(q_out[start:end], p3, start)))

    kept = shared_expert(normed, own_out, shared_gate, shared_up, shared_down)
    return finish(kept, outer, inner, resid1, post_gain)


PIECES = 4
INNER = ((0, 2), (2, 4))


def edge_product(x_in, gate_c, edge):
    row_count, channels = x_in.shape
    tile = 2 * edge

    def kernel(x_ref, c_ref, out_ref):
        product = c_ref[...].astype(f32) * x_ref[...].astype(f32)
        out_ref[...] = product[tile - edge :]

    last = pl.BlockSpec((tile, channels), lambda i: (row_count // tile - 1, 0))
    return pl.pallas_call(
        kernel,
        grid=(1,),
        out_shape=jax.ShapeDtypeStruct((edge, channels), f32),
        in_specs=[last, last],
        out_specs=pl.BlockSpec((edge, channels), lambda i: (0, 0)),
        cost_estimate=cost(4 * MIB),
        name="edge_product",
    )(x_in, gate_c)


def expert_parts(gate_w, up_w, part, spans, count, *down_w):
    depth = max(end for _, end in spans)

    def kernel(*refs):
        ins, outs = refs[: 2 * count + len(down_w)], refs[2 * count + len(down_w) :]
        for i, ref in enumerate(ins[: 2 * count]):
            for (start, end), out in zip(spans, outs):
                out[:, i * part : (i + 1) * part] = ref[start:end]
        if down_w:
            outs[-1][...] = ins[-1][...]

    specs = [
        pl.BlockSpec((depth, part), lambda i, f=flipped: (0, lax.axis_index("tp") ^ f))
        for flipped in range(0, 2 * count, 2)
        for _ in range(2)
    ]
    shapes = [(end - start, 2 * count * part) for start, end in spans]
    for down in down_w:
        specs.append(pl.BlockSpec((part, down.shape[1]), lambda i: (lax.axis_index("tp"), 0)))
        shapes.append((part, down.shape[1]))
    return pl.pallas_call(
        kernel,
        grid=(1,),
        out_shape=[jax.ShapeDtypeStruct(shape, bf16) for shape in shapes],
        in_specs=specs,
        out_specs=[pl.BlockSpec(shape, lambda i: (0, 0)) for shape in shapes],
        cost_estimate=cost(4 * MIB),
        compiler_params=pltpu.CompilerParams(vmem_limit_bytes=(16 if down_w else 60) * MIB),
        name="parts",
    )(*[gate_w, up_w] * count, *down_w)


def convolve(x_in, gate_b, gate_c, conv_taps, edge, rows):
    row_count, channels = x_in.shape
    reach = conv_taps.shape[0] - 1
    groups = row_count // rows

    def kernel(x_ref, g_ref, b_ref, taps_ref, mine, give, head, head_gate, before):
        group = pl.program_id(0)
        core = lax.axis_index("tp") % 2
        taps = taps_ref[...].astype(f32)
        mixed = g_ref[...].astype(f32) * x_ref[...].astype(f32)
        gate = b_ref[...].astype(f32)

        @pl.when(group == 0)
        def _():
            before[...] = jnp.zeros((edge, channels), f32)

        padded = jnp.concatenate([before[...], mixed], 0)
        before[...] = mixed[rows - edge :]
        total = jnp.zeros((rows, channels), f32)
        for index in range(reach + 1):
            start = edge - reach + index
            total = total + taps[index : index + 1] * padded[start : start + rows]
        result = (gate * total).astype(bf16)

        @pl.when(group == 0)
        def _():
            head[...] = total[:edge]
            head_gate[...] = gate[:edge]

        @pl.when(core == group % 2)
        def _():
            mine[group // 2] = result

        @pl.when(core != group % 2)
        def _():
            give[group // 2] = result

    shape = ((groups // 2, rows, channels), bf16)
    small = ((edge, channels), f32)
    shapes = [shape, shape, small, small]
    block = pl.BlockSpec((rows, channels), lambda i: (i, 0))
    return pl.pallas_call(
        kernel,
        grid=(groups,),
        out_shape=[jax.ShapeDtypeStruct(*s) for s in shapes],
        in_specs=[block] * 3 + [pl.BlockSpec(conv_taps.shape, lambda i: (0, 0))],
        out_specs=[pl.BlockSpec(s[0], lambda i, n=len(s[0]): (0,) * n) for s in shapes],
        scratch_shapes=[pltpu.VMEM((edge, channels), f32)],
        compiler_params=pltpu.CompilerParams(vmem_limit_bytes=8 * MIB),
        name="convolve",
    )(x_in, gate_c, gate_b, conv_taps)


def convolve_edge(edge_in, conv_taps, mine, give, head, head_gate):
    edge, channels = edge_in.shape
    reach = conv_taps.shape[0] - 1

    def kernel(edge_ref, taps_ref, mine_ref, give_ref, head_ref, gate_ref, mine_out, give_out):
        core = lax.axis_index("tp") % 2
        taps = taps_ref[...].astype(f32)
        before = jnp.where(lax.axis_index("sp") > 0, edge_ref[...], 0.0)
        padded = jnp.concatenate([before, jnp.zeros((edge, channels), f32)], 0)
        total = jnp.zeros((edge, channels), f32)
        for index in range(reach):
            start = edge - reach + index
            total = total + taps[index : index + 1] * padded[start : start + edge]
        result = (gate_ref[...] * (total + head_ref[...])).astype(bf16)
        mine_out[...] = mine_ref[...]
        give_out[...] = give_ref[...]

        @pl.when(core == 0)
        def _():
            mine_out[0, :edge] = result

        @pl.when(core != 0)
        def _():
            give_out[0, :edge] = result

    shape = (mine.shape, bf16)
    operands = (edge_in, conv_taps, mine, give, head, head_gate)
    return call(kernel, [shape, shape], *operands, limit=4)


def project(other, mine, got, proj, proj_other, dtype):
    rows = mine.shape[1]
    width = proj.shape[1]

    def kernel(mine_ref, got_ref, proj_ref, other_ref, out_ref):
        y = lax.axis_index("tp") // 2
        y = 1 - y if other else y
        a, b = mine_ref[y], got_ref[y]
        step = 512
        for n in range(0, width, step):
            cols = slice(n, n + step)
            out_ref[:, cols] = (dot(a, proj_ref[:, cols]) + dot(b, other_ref[:, cols])).astype(dtype)

    flops = 4 * rows * proj.size
    return call(kernel, [((rows, width), dtype)], mine, got, proj, proj_other, flops=flops)


PARTS = 3


def route_table(routes, weights, experts):
    top, rows = routes.shape
    lanes = 128

    def kernel(routes_ref, weights_ref, out_ref):
        expert = lax.broadcasted_iota(jnp.int32, (experts, rows), 0)
        left = jnp.zeros((experts, rows), f32)
        for k in range(top):
            left = left + jnp.where(routes_ref[k : k + 1] == expert, weights_ref[k : k + 1], 0.0)
        pieces = []
        for _ in range(PARTS):
            piece = left.astype(bf16).astype(f32)
            left = left - piece
            pieces.append(piece)
        pieces.append(jnp.zeros((lanes - PARTS * experts, rows), f32))
        out_ref[...] = jnp.concatenate(pieces, 0).T.astype(bf16)

    return call(kernel, [((rows, lanes), bf16)], routes, weights, limit=4)


def norms(near, far_in, resid, mix_gain, pre_gain):
    rows, width = near.shape
    half = width // 2
    step = 32

    def kernel(near_ref, far_ref, resid_ref, mix_ref, pre_ref, resid_out, *normed_out):
        mix, pre = mix_ref[...].astype(f32), pre_ref[...].astype(f32)
        for r in range(0, rows, step):
            span = slice(r, r + step)
            total = near_ref[span] + far_ref[span].astype(f32)
            scale = lax.rsqrt(jnp.mean(total * total, axis=1, keepdims=True) + epsilon)
            row = (resid_ref[span].astype(f32) + total * scale * mix).astype(bf16)
            resid_out[span] = row
            wide = row.astype(f32)
            scale = lax.rsqrt(jnp.mean(wide * wide, axis=1, keepdims=True) + epsilon)
            normed = (wide * scale * pre).astype(bf16)
            for i, out in enumerate(normed_out):
                out[span] = normed[:, i * half : (i + 1) * half]

    operands = (near, far_in, resid, mix_gain[None], pre_gain[None])
    shapes = [((rows, width), bf16)] + [((rows, half), bf16)] * 2
    return call(kernel, shapes, *operands)


def added(outs, back, first=0):
    rows, piece = outs[0].shape
    count = len(outs)

    def kernel(*refs):
        back_ref, sum_ref = refs[count:]
        for i, ref in enumerate(refs[:count]):
            start = (first + i) * piece
            back_part = jnp.where(in_middle(), back_ref[:, start : start + piece].astype(f32), 0.0)
            sum_ref[:, i * piece : (i + 1) * piece] = (ref[...].astype(f32) + back_part).astype(bf16)

    return call(kernel, [((rows, count * piece), bf16)], *outs, back, limit=4)


def shared_expert(normed, own, gate, up, down):
    rows = normed[0].shape[0]
    width = gate.shape[0]
    step = own[0].shape[1]

    def kernel(*refs):
        block = jnp.concatenate([ref[...] for ref in refs[: len(normed)]], 1)
        refs = refs[len(normed) :]
        gate_ref, up_ref, down_ref, out_ref = refs[len(own) :]
        hidden = (silu(dot(block, gate_ref[...])) * dot(block, up_ref[...])).astype(bf16)
        for i, ref in enumerate(refs[: len(own)]):
            cols = slice(i * step, (i + 1) * step)
            out_ref[:, cols] = ref[...].astype(f32) + dot(hidden, down_ref[:, cols])

    flops = 6 * rows * gate.size
    operands = (*normed, *own, gate, up, down)
    return call(kernel, [((rows, width), f32)], *operands, flops=flops)


def finish(kept, outer, inner, resid1, gain):
    rows, width = kept.shape
    piece = outer[0].shape[1]
    places = [(k, i - a) for k, (a, b) in enumerate(INNER) for i in range(a, b)]
    step = 64

    def kernel(kept_ref, *refs):
        outer_refs, inner_refs = refs[: len(outer)], refs[len(outer) : len(outer) + len(inner)]
        resid_ref, gain_ref, out_ref = refs[len(outer) + len(inner) :]
        middle = in_middle()
        parts, square = [], 0.0
        for i, ref in enumerate(outer_refs):
            part = kept_ref[:, i * piece : (i + 1) * piece] + ref[...].astype(f32)
            which, place = places[i]
            back = inner_refs[which][:, place * piece : (place + 1) * piece].astype(f32)
            part = part + jnp.where(middle, back, 0.0)
            square = square + jnp.sum(part * part, axis=1, keepdims=True)
            parts.append(part)
        factor = lax.rsqrt(square * (1.0 / width) + epsilon)
        for i, part in enumerate(parts):
            cols = slice(i * piece, (i + 1) * piece)
            scaled = part * factor * gain_ref[:, cols].astype(f32)
            out_ref[:, cols] = (resid_ref[:, cols].astype(f32) + scaled).astype(bf16)

    def block(array):
        return pl.BlockSpec((step, array.shape[1]), lambda i: (i, 0))

    operands = (kept, *outer, *inner, resid1)
    return pl.pallas_call(
        kernel,
        grid=(rows // step,),
        out_shape=jax.ShapeDtypeStruct((rows, width), bf16),
        in_specs=[block(x) for x in operands] + [pl.BlockSpec((1, width), lambda i: (0, 0))],
        out_specs=block(kept),
        compiler_params=pltpu.CompilerParams(vmem_limit_bytes=8 * MIB),
        name="finish",
    )(*operands, gain[None])


def block_of(refs):
    if len(refs) == 1:
        return refs[0][...]
    return jnp.where(in_middle(), refs[0][...], refs[1][...])


def gather_blocks(refs, blocks):
    rows, refs = [], list(refs)
    for block in blocks:
        pieces = []
        for piece in block:
            pieces.append(block_of([refs.pop(0) for _ in piece]))
        rows.append(pieces[0] if len(pieces) == 1 else jnp.concatenate(pieces, 1))
    return rows[0] if len(rows) == 1 else jnp.concatenate(rows, 0)


def scale_of(table, expert, experts):
    lane = lax.broadcasted_iota(jnp.int32, table.shape, 1)
    chosen = jnp.where(lane % experts == expert, table.astype(f32), 0.0)
    return jnp.sum(chosen, axis=1, keepdims=True)


def run_pair(blocks, tables, sends, gate, up, down, *others, ends=False):
    experts = lax.axis_size("sp")
    inputs = [array for block in blocks for piece in block for array in piece]
    inputs_t = [array for block in tables for piece in block for array in piece]
    count = len(inputs) + len(inputs_t)
    rows = inputs[0].shape[0]
    hidden_size, width = down.shape

    def kernel(*refs):
        if ends:

            @pl.when(~in_middle())
            def _():
                compute(*refs)

        else:
            compute(*refs)

    def compute(*refs):
        gate_ref, up_ref, down_ref = refs[count : count + 3]
        g1a, g1b, g1c, g1d, da, db, dc, dd, g2a, g2c, g3a, g3c = refs[count + 3 : count + 15]
        outs = refs[count + 15 :]
        part, half = da.shape[0], g1a.shape[0]
        cut = half + g2a.shape[0]
        block = gather_blocks(refs[: len(inputs)], blocks)
        table = gather_blocks(refs[len(inputs) : count], tables)
        own = lax.axis_index("sp")
        scale = scale_of(table, own, experts)
        hidden = []
        for i in range(0, hidden_size, 2 * part):
            g = dot(block, gate_ref[:, i : i + 2 * part])
            u = dot(block, up_ref[:, i : i + 2 * part])
            hidden.append((silu(g) * u * scale).astype(bf16))
        scale = scale_of(table, own ^ 1, experts)
        rest = []
        for i, top in enumerate((g1a, g1b, g1c, g1d)):
            side = (i % 2) * 2 * part
            gu = dot(block[:, :half], top[...])
            gu += dot(block[:, half:cut], (g2a, g2c)[i // 2][:, side : side + 2 * part])
            gu += dot(block[:, cut:], (g3a, g3c)[i // 2][:, side : side + 2 * part])
            rest.append((silu(gu[:, :part]) * gu[:, part:] * scale).astype(bf16))
        hidden.append(jnp.concatenate(rest[:2], 1))
        hidden.append(jnp.concatenate(rest[2:], 1))
        step = 512
        for n in range(0, width, step):
            cols = slice(n, n + step)
            total = dot(hidden[0], down_ref[0 : 2 * part, cols])
            total += dot(hidden[1], down_ref[2 * part : 4 * part, cols])
            total += dot(hidden[2], jnp.concatenate([da[:, cols], db[:, cols]], 0))
            total += dot(hidden[3], jnp.concatenate([dc[:, cols], dd[:, cols]], 0))
            total = total.astype(bf16)
            piece, start = n // (width // PIECES), n % (width // PIECES)
            for i in range(len(blocks)):
                out = outs[PIECES * i + piece]
                out[:, start : start + step] = total[i * rows : (i + 1) * rows]
            if sends:
                outs[-1][:, cols] = jnp.where(in_middle(), block[:, cols], total)

    flops = 12 * len(blocks) * rows * width * hidden_size
    shapes = [((rows, width // PIECES), bf16)] * (PIECES * len(blocks))
    if sends:
        shapes.append(((rows, width), bf16))
    operands = [*inputs, *inputs_t, gate, up, down, *others]
    limit = 4 + 6 * len(blocks)
    return call(kernel, shapes, *operands, limit=limit, flops=flops)


def layer(*args):
    return dense_body(*args)


def solution(mesh):
    few = mesh.shape["sp"] == 8 and mesh.shape["tp"] == 4
    return jax.shard_map(
        layer if few else routed_body,
        mesh=mesh,
        in_specs=(
            P("sp", "tp"),
            P("sp", "tp"),
            P("sp", "tp"),
            P(None, "tp"),
            P("tp", None),
            P(),
            P(("sp", "tp"), None),
            P(),
            P("sp", None, None),
            P("sp", None, None),
            P("sp", None, None),
            P(),
            P(),
            P(),
            P(),
            P(("sp", "tp"), None),
            P(("sp", "tp"), None),
        ),
        out_specs=P(("sp", "tp"), None),
        check_vma=False,
    )
```

```python
import jax
import jax.numpy as jnp
from jax import lax
from jax.experimental import pallas as pl
from jax.experimental.pallas import tpu as pltpu
from jax.sharding import PartitionSpec as P

epsilon = 1e-06
f32 = jnp.float32
bf16 = jnp.bfloat16
MIB = 1024 * 1024


def passed_along(shard, axis, by):
    size = lax.axis_size(axis)
    pairs = [(i, i + by) for i in range(size) if 0 <= i + by < size]
    return lax.ppermute(shard, axis, pairs)


def routed_body(
    x_in,
    gate_b,
    gate_c,
    conv_taps,
    out_proj,
    mix_gain,
    resid,
    pre_gain,
    expert_gate,
    expert_up,
    expert_down,
    shared_gate,
    shared_up,
    shared_down,
    post_gain,
    routes,
    route_weights,
):
    row_count = x_in.shape[0]
    channels = x_in.shape[1]
    reach = conv_taps.shape[0] - 1
    edge_rows = jnp.concatenate([x_in[row_count - reach :], gate_c[row_count - reach :]], 1)
    arrived_edge = passed_along(edge_rows, "sp", 1)
    inputs = jnp.concatenate([arrived_edge[:, :channels], x_in], 0).astype(jnp.float32)
    gate_rows = jnp.concatenate([arrived_edge[:, channels:], gate_c], 0).astype(jnp.float32)
    mixed_in = inputs * gate_rows
    taps = conv_taps.astype(jnp.float32)
    convolved = jnp.zeros((row_count, channels), jnp.float32)
    for index in range(reach + 1):
        convolved = convolved + taps[index][None, :] * mixed_in[index : index + row_count]
    conv_out = (gate_b.astype(jnp.float32) * convolved).astype(jnp.bfloat16)
    width_all = out_proj.shape[1]
    full_rows = lax.all_to_all(conv_out, "tp", split_axis=0, concat_axis=1, tiled=True)
    projected = jnp.dot(
        full_rows,
        lax.all_gather(out_proj, "tp", axis=0, tiled=True),
        preferred_element_type=jnp.float32,
    )
    row_scale = lax.rsqrt(jnp.mean(projected * projected, axis=1, keepdims=True) + epsilon)
    resid1 = (
        resid.astype(jnp.float32) + projected * row_scale * mix_gain.astype(jnp.float32)
    ).astype(jnp.bfloat16)
    wide_resid = resid1.astype(jnp.float32)
    normed = (
        wide_resid
        * lax.rsqrt(jnp.mean(wide_resid * wide_resid, axis=1, keepdims=True) + epsilon)
        * pre_gain.astype(jnp.float32)
    ).astype(jnp.bfloat16)
    experts = lax.axis_size("sp")
    local_rows = resid.shape[0]
    top_count = routes.shape[1]
    capacity = 3 * local_rows * top_count // (2 * experts)
    flat_ids = routes.reshape(-1)
    onehot = (flat_ids[:, None] == jnp.arange(experts, dtype=jnp.int32)[None, :]).astype(jnp.int32)
    before = jnp.cumsum(onehot, axis=0) - onehot
    position = jnp.sum(before * onehot, axis=1)
    slot_index = flat_ids * capacity + position
    outgoing = (
        jnp.zeros((experts * capacity, width_all), jnp.bfloat16)
        .at[slot_index]
        .set(jnp.repeat(normed, top_count, axis=0))
    )
    received = lax.all_to_all(
        outgoing.reshape(experts, capacity, width_all),
        "sp",
        split_axis=0,
        concat_axis=0,
        tiled=True,
    )
    arrived = received.reshape(experts * capacity, width_all)
    gate_h = jnp.dot(arrived, expert_gate[0], preferred_element_type=jnp.float32)
    up_h = jnp.dot(arrived, expert_up[0], preferred_element_type=jnp.float32)
    hidden = (jax.nn.silu(gate_h) * up_h).astype(jnp.bfloat16)
    expert_out = jnp.dot(hidden, expert_down[0], preferred_element_type=jnp.float32).astype(
        jnp.bfloat16
    )
    returned = lax.all_to_all(
        expert_out.reshape(experts, capacity, width_all),
        "sp",
        split_axis=0,
        concat_axis=0,
        tiled=True,
    )
    returned = returned.reshape(experts * capacity, width_all)
    picked = returned[slot_index].astype(jnp.float32).reshape(local_rows, top_count, width_all)
    routed = jnp.einsum("tk,tkd->td", route_weights, picked)
    shared_g = jnp.dot(normed, shared_gate, preferred_element_type=jnp.float32)
    shared_u = jnp.dot(normed, shared_up, preferred_element_type=jnp.float32)
    shared_hidden = (jax.nn.silu(shared_g) * shared_u).astype(jnp.bfloat16)
    shared_out = jnp.dot(shared_hidden, shared_down, preferred_element_type=jnp.float32)
    branch = routed + shared_out
    factor = lax.rsqrt(jnp.mean(branch * branch, axis=1, keepdims=True) + epsilon)
    return (wide_resid + branch * factor * post_gain.astype(jnp.float32)[None, :]).astype(
        jnp.bfloat16
    )


def dot(a, b):
    return jnp.dot(a, b, preferred_element_type=f32)


def silu(g):
    return g * jax.nn.sigmoid(g)


def flip(array, axis, bit):
    return lax.ppermute(array, axis, [(i, i ^ bit) for i in range(lax.axis_size(axis))])


def middle_swap(array):
    size, inner = lax.axis_size("sp"), lax.axis_size("tp")
    quarter = size // 4
    pairs = []
    for i in range(size):
        end = i < quarter or i >= 3 * quarter
        for j in range(inner):
            target = (i, j ^ 1) if end else (i ^ (3 * quarter), j)
            pairs.append((i * inner + j, target[0] * inner + target[1]))
    return lax.ppermute(array, ("sp", "tp"), pairs)


def in_middle():
    z = lax.axis_index("sp") // 2
    return (z > 0) & (z < lax.axis_size("sp") // 2 - 1)


VMEM = pl.BlockSpec(memory_space=pltpu.VMEM)


def cost(moved, flops=0):
    return pl.CostEstimate(flops=flops, bytes_accessed=moved, transcendentals=0)


def call(kernel, out_shape, *operands, limit=8, flops=0):
    shapes = [jax.ShapeDtypeStruct(*shape) for shape in out_shape]
    out = pl.pallas_call(
        kernel,
        out_shape=shapes,
        in_specs=[VMEM] * len(operands),
        out_specs=[VMEM] * len(shapes),
        cost_estimate=cost(MIB, flops),
        compiler_params=pltpu.CompilerParams(vmem_limit_bytes=limit * MIB),
    )(*operands)
    return out[0] if len(out) == 1 else out


def dense_body(
    x_in,
    gate_b,
    gate_c,
    conv_taps,
    out_proj,
    mix_gain,
    resid,
    pre_gain,
    expert_gate,
    expert_up,
    expert_down,
    shared_gate,
    shared_up,
    shared_down,
    post_gain,
    routes,
    route_weights,
):
    tp_size = lax.axis_size("tp")
    rows = resid.shape[0]
    edge = 8

    edge_rows = edge_product(x_in, gate_c, edge)
    size = lax.axis_size("sp")
    edge_in = lax.ppermute(edge_rows, "sp", [(i, (i + 1) % size) for i in range(size)])
    rest = convolve(x_in, gate_b, gate_c, conv_taps, edge, rows)
    mine, give = convolve_edge(edge_in, conv_taps, *rest)

    proj_other = flip(out_proj, "tp", 1)

    got = flip(give, "tp", 1)
    far = project(1, mine, got, out_proj, proj_other, bf16)
    far_in = flip(far, "tp", 2)
    near = project(0, mine, got, out_proj, proj_other, f32)
    table = route_table(routes.T, route_weights.T, lax.axis_size("sp"))
    resid1, *normed = norms(near, far_in, resid, mix_gain, pre_gain)

    gate_w, up_w, down_w = expert_gate[0], expert_up[0], expert_down[0]
    part = gate_w.shape[1] // tp_size
    depth = gate_w.shape[0]
    head, cut = depth * 5 // 8, depth * 7 // 8
    (g1,) = expert_parts(gate_w, up_w, part, [(0, head)], 1)
    spans = [(head, cut), (cut, depth)]
    g2, g3, dn = expert_parts(gate_w, up_w, part, spans, 2, down_w)
    others = []
    for piece in (g1, dn):
        piece_a = flip(piece, "sp", 1)
        piece_b = flip(piece_a, "tp", 2)
        piece_c = flip(piece_a, "tp", 1)
        piece_d = flip(piece_b, "tp", 1)
        others += [piece_a, piece_b, piece_c, piece_d]
    for piece in (g2, g3):
        piece_a = flip(piece, "sp", 1)
        others += [piece_a, flip(piece_a, "tp", 1)]

    p1_table = flip(table, "sp", 2)
    q1_table = middle_swap(table)
    q2_table = middle_swap(p1_table)
    p2_table = flip(q1_table, "sp", 2)
    p3_table = flip(q2_table, "sp", 2)
    p1, q1, q2, p2 = [], [], [], []
    for i, piece in enumerate(normed):
        p1.append(flip(piece, "sp", 2))
        q1.append(middle_swap(piece))
        q2.append(middle_swap(p1[i]))
        p2.append(flip(q1[i], "sp", 2))

    weights = (gate_w, up_w, down_w, *others)
    two_tables = [[(q2_table, p2_table)]]
    *two_out, send, tail = run_pair([list(zip(q2, p2))], two_tables, True, *weights)
    p3_a = flip(q2[0], "sp", 2)
    p3_b = flip(send, "sp", 2)
    e2_b = flip(tail, "sp", 2)
    near_blocks = [list(zip(pieces)) for pieces in (normed, p1, q1)]
    near_tables = [[(t,)] for t in (table, p1_table, q1_table)]
    near_out = run_pair(near_blocks, near_tables, False, *weights)
    own_out, p_out, q_out = (near_out[i * PIECES : (i + 1) * PIECES] for i in range(3))
    three_out = run_pair([[(p3_a,), (p3_b,)]], [[(p3_table,)]], False, *weights, ends=True)

    outer, inner = [], []
    for i in range(PIECES):
        r1 = flip(three_out[i], "sp", 2)
        m2 = middle_swap(added([two_out[i]], r1))
        outer.append(flip(added([p_out[i]], m2), "sp", 2))
    for i, (start, end) in enumerate(INNER):
        inner.append(middle_swap(added(q_out[start:end], (p3_b, e2_b)[i])))

    kept = shared_expert(normed, own_out, shared_gate, shared_up, shared_down)
    return finish(kept, outer, inner, resid1, post_gain)


PIECES = 4
INNER = ((0, 2), (2, 4))


def edge_product(x_in, gate_c, edge):
    row_count, channels = x_in.shape
    tile = 2 * edge

    def kernel(x_ref, c_ref, out_ref):
        product = c_ref[...].astype(f32) * x_ref[...].astype(f32)
        out_ref[...] = product[tile - edge :]

    last = pl.BlockSpec((tile, channels), lambda i: (row_count // tile - 1, 0))
    return pl.pallas_call(
        kernel,
        grid=(1,),
        out_shape=jax.ShapeDtypeStruct((edge, channels), f32),
        in_specs=[last, last],
        out_specs=pl.BlockSpec((edge, channels), lambda i: (0, 0)),
        cost_estimate=cost(4 * MIB),
        name="edge_product",
    )(x_in, gate_c)


def expert_parts(gate_w, up_w, part, spans, count, *down_w):
    depth = max(end for _, end in spans)

    def kernel(*refs):
        ins, outs = refs[: 2 * count + len(down_w)], refs[2 * count + len(down_w) :]
        for i, ref in enumerate(ins[: 2 * count]):
            for (start, end), out in zip(spans, outs):
                out[:, i * part : (i + 1) * part] = ref[start:end]
        if down_w:
            outs[-1][...] = ins[-1][...]

    specs = [
        pl.BlockSpec((depth, part), lambda i, f=flipped: (0, lax.axis_index("tp") ^ f))
        for flipped in range(0, 2 * count, 2)
        for _ in range(2)
    ]
    shapes = [(end - start, 2 * count * part) for start, end in spans]
    for down in down_w:
        specs.append(pl.BlockSpec((part, down.shape[1]), lambda i: (lax.axis_index("tp"), 0)))
        shapes.append((part, down.shape[1]))
    return pl.pallas_call(
        kernel,
        grid=(1,),
        out_shape=[jax.ShapeDtypeStruct(shape, bf16) for shape in shapes],
        in_specs=specs,
        out_specs=[pl.BlockSpec(shape, lambda i: (0, 0)) for shape in shapes],
        cost_estimate=cost(4 * MIB),
        compiler_params=pltpu.CompilerParams(vmem_limit_bytes=(16 if down_w else 60) * MIB),
        name="parts",
    )(*[gate_w, up_w] * count, *down_w)


def convolve(x_in, gate_b, gate_c, conv_taps, edge, rows):
    row_count, channels = x_in.shape
    reach = conv_taps.shape[0] - 1
    groups = row_count // rows

    def kernel(x_ref, g_ref, b_ref, taps_ref, mine, give, head, head_gate, before):
        group = pl.program_id(0)
        core = lax.axis_index("tp") % 2
        taps = taps_ref[...].astype(f32)
        mixed = g_ref[...].astype(f32) * x_ref[...].astype(f32)
        gate = b_ref[...].astype(f32)

        @pl.when(group == 0)
        def _():
            before[...] = jnp.zeros((edge, channels), f32)

        padded = jnp.concatenate([before[...], mixed], 0)
        before[...] = mixed[rows - edge :]
        total = jnp.zeros((rows, channels), f32)
        for index in range(reach + 1):
            start = edge - reach + index
            total = total + taps[index : index + 1] * padded[start : start + rows]
        result = (gate * total).astype(bf16)

        @pl.when(group == 0)
        def _():
            head[...] = total[:edge]
            head_gate[...] = gate[:edge]

        @pl.when(core == group % 2)
        def _():
            mine[group // 2] = result

        @pl.when(core != group % 2)
        def _():
            give[group // 2] = result

    shape = ((groups // 2, rows, channels), bf16)
    small = ((edge, channels), f32)
    shapes = [shape, shape, small, small]
    block = pl.BlockSpec((rows, channels), lambda i: (i, 0))
    return pl.pallas_call(
        kernel,
        grid=(groups,),
        out_shape=[jax.ShapeDtypeStruct(*s) for s in shapes],
        in_specs=[block] * 3 + [pl.BlockSpec(conv_taps.shape, lambda i: (0, 0))],
        out_specs=[pl.BlockSpec(s[0], lambda i, n=len(s[0]): (0,) * n) for s in shapes],
        scratch_shapes=[pltpu.VMEM((edge, channels), f32)],
        compiler_params=pltpu.CompilerParams(vmem_limit_bytes=8 * MIB),
        name="convolve",
    )(x_in, gate_c, gate_b, conv_taps)


def convolve_edge(edge_in, conv_taps, mine, give, head, head_gate):
    edge, channels = edge_in.shape
    reach = conv_taps.shape[0] - 1

    def kernel(edge_ref, taps_ref, mine_ref, give_ref, head_ref, gate_ref, mine_out, give_out):
        core = lax.axis_index("tp") % 2
        taps = taps_ref[...].astype(f32)
        before = jnp.where(lax.axis_index("sp") > 0, edge_ref[...], 0.0)
        padded = jnp.concatenate([before, jnp.zeros((edge, channels), f32)], 0)
        total = jnp.zeros((edge, channels), f32)
        for index in range(reach):
            start = edge - reach + index
            total = total + taps[index : index + 1] * padded[start : start + edge]
        result = (gate_ref[...] * (total + head_ref[...])).astype(bf16)
        mine_out[...] = mine_ref[...]
        give_out[...] = give_ref[...]

        @pl.when(core == 0)
        def _():
            mine_out[0, :edge] = result

        @pl.when(core != 0)
        def _():
            give_out[0, :edge] = result

    shape = (mine.shape, bf16)
    operands = (edge_in, conv_taps, mine, give, head, head_gate)
    return call(kernel, [shape, shape], *operands, limit=4)


def project(other, mine, got, proj, proj_other, dtype):
    rows = mine.shape[1]
    width = proj.shape[1]

    def kernel(mine_ref, got_ref, proj_ref, other_ref, out_ref):
        y = lax.axis_index("tp") // 2
        y = 1 - y if other else y
        a, b = mine_ref[y], got_ref[y]
        step = 512
        for n in range(0, width, step):
            cols = slice(n, n + step)
            out_ref[:, cols] = (dot(a, proj_ref[:, cols]) + dot(b, other_ref[:, cols])).astype(dtype)

    flops = 4 * rows * proj.size
    return call(kernel, [((rows, width), dtype)], mine, got, proj, proj_other, flops=flops)


PARTS = 3


def route_table(routes, weights, experts):
    top, rows = routes.shape
    lanes = 128

    def kernel(routes_ref, weights_ref, out_ref):
        expert = lax.broadcasted_iota(jnp.int32, (experts, rows), 0)
        left = jnp.zeros((experts, rows), f32)
        for k in range(top):
            left = left + jnp.where(routes_ref[k : k + 1] == expert, weights_ref[k : k + 1], 0.0)
        pieces = []
        for _ in range(PARTS):
            piece = left.astype(bf16).astype(f32)
            left = left - piece
            pieces.append(piece)
        pieces.append(jnp.zeros((lanes - PARTS * experts, rows), f32))
        out_ref[...] = jnp.concatenate(pieces, 0).T.astype(bf16)

    return call(kernel, [((rows, lanes), bf16)], routes, weights, limit=4)


def norms(near, far_in, resid, mix_gain, pre_gain):
    rows, width = near.shape
    half = width // 2
    step = 32

    def kernel(near_ref, far_ref, resid_ref, mix_ref, pre_ref, resid_out, *normed_out):
        mix, pre = mix_ref[...].astype(f32), pre_ref[...].astype(f32)
        for r in range(0, rows, step):
            span = slice(r, r + step)
            total = near_ref[span] + far_ref[span].astype(f32)
            scale = lax.rsqrt(jnp.mean(total * total, axis=1, keepdims=True) + epsilon)
            row = (resid_ref[span].astype(f32) + total * scale * mix).astype(bf16)
            resid_out[span] = row
            wide = row.astype(f32)
            scale = lax.rsqrt(jnp.mean(wide * wide, axis=1, keepdims=True) + epsilon)
            normed = (wide * scale * pre).astype(bf16)
            for i, out in enumerate(normed_out):
                out[span] = normed[:, i * half : (i + 1) * half]

    operands = (near, far_in, resid, mix_gain[None], pre_gain[None])
    shapes = [((rows, width), bf16)] + [((rows, half), bf16)] * 2
    return call(kernel, shapes, *operands)


def added(outs, back, first=0):
    rows, piece = outs[0].shape
    count = len(outs)

    def kernel(*refs):
        back_ref, sum_ref = refs[count:]
        for i, ref in enumerate(refs[:count]):
            start = (first + i) * piece
            back_part = jnp.where(in_middle(), back_ref[:, start : start + piece].astype(f32), 0.0)
            sum_ref[:, i * piece : (i + 1) * piece] = (ref[...].astype(f32) + back_part).astype(bf16)

    return call(kernel, [((rows, count * piece), bf16)], *outs, back, limit=4)


def shared_expert(normed, own, gate, up, down):
    rows = normed[0].shape[0]
    width = gate.shape[0]
    step = own[0].shape[1]

    def kernel(*refs):
        block = jnp.concatenate([ref[...] for ref in refs[: len(normed)]], 1)
        refs = refs[len(normed) :]
        gate_ref, up_ref, down_ref, out_ref = refs[len(own) :]
        hidden = (silu(dot(block, gate_ref[...])) * dot(block, up_ref[...])).astype(bf16)
        for i, ref in enumerate(refs[: len(own)]):
            cols = slice(i * step, (i + 1) * step)
            out_ref[:, cols] = ref[...].astype(f32) + dot(hidden, down_ref[:, cols])

    flops = 6 * rows * gate.size
    operands = (*normed, *own, gate, up, down)
    return call(kernel, [((rows, width), f32)], *operands, flops=flops)


def finish(kept, outer, inner, resid1, gain):
    rows, width = kept.shape
    piece = outer[0].shape[1]
    places = [(k, i - a) for k, (a, b) in enumerate(INNER) for i in range(a, b)]
    step = 64

    def kernel(kept_ref, *refs):
        outer_refs, inner_refs = refs[: len(outer)], refs[len(outer) : len(outer) + len(inner)]
        resid_ref, gain_ref, out_ref = refs[len(outer) + len(inner) :]
        middle = in_middle()
        parts, square = [], 0.0
        for i, ref in enumerate(outer_refs):
            part = kept_ref[:, i * piece : (i + 1) * piece] + ref[...].astype(f32)
            which, place = places[i]
            back = inner_refs[which][:, place * piece : (place + 1) * piece].astype(f32)
            part = part + jnp.where(middle, back, 0.0)
            square = square + jnp.sum(part * part, axis=1, keepdims=True)
            parts.append(part)
        factor = lax.rsqrt(square * (1.0 / width) + epsilon)
        for i, part in enumerate(parts):
            cols = slice(i * piece, (i + 1) * piece)
            scaled = part * factor * gain_ref[:, cols].astype(f32)
            out_ref[:, cols] = (resid_ref[:, cols].astype(f32) + scaled).astype(bf16)

    def block(array):
        return pl.BlockSpec((step, array.shape[1]), lambda i: (i, 0))

    operands = (kept, *outer, *inner, resid1)
    return pl.pallas_call(
        kernel,
        grid=(rows // step,),
        out_shape=jax.ShapeDtypeStruct((rows, width), bf16),
        in_specs=[block(x) for x in operands] + [pl.BlockSpec((1, width), lambda i: (0, 0))],
        out_specs=block(kept),
        compiler_params=pltpu.CompilerParams(vmem_limit_bytes=8 * MIB),
        name="finish",
    )(*operands, gain[None])


def block_of(refs):
    if len(refs) == 1:
        return refs[0][...]
    return jnp.where(in_middle(), refs[0][...], refs[1][...])


def gather_blocks(refs, blocks):
    rows, refs = [], list(refs)
    for block in blocks:
        pieces = []
        for piece in block:
            pieces.append(block_of([refs.pop(0) for _ in piece]))
        rows.append(pieces[0] if len(pieces) == 1 else jnp.concatenate(pieces, 1))
    return rows[0] if len(rows) == 1 else jnp.concatenate(rows, 0)


def scale_of(table, expert, experts):
    lane = lax.broadcasted_iota(jnp.int32, table.shape, 1)
    chosen = jnp.where(lane % experts == expert, table.astype(f32), 0.0)
    return jnp.sum(chosen, axis=1, keepdims=True)


def run_pair(blocks, tables, sends, gate, up, down, *others, ends=False):
    experts = lax.axis_size("sp")
    inputs = [array for block in blocks for piece in block for array in piece]
    inputs_t = [array for block in tables for piece in block for array in piece]
    count = len(inputs) + len(inputs_t)
    rows = inputs[0].shape[0]
    hidden_size, width = down.shape

    def kernel(*refs):
        if ends:

            @pl.when(~in_middle())
            def _():
                compute(*refs)

        else:
            compute(*refs)

    def compute(*refs):
        gate_ref, up_ref, down_ref = refs[count : count + 3]
        g1a, g1b, g1c, g1d, da, db, dc, dd, g2a, g2c, g3a, g3c = refs[count + 3 : count + 15]
        outs = refs[count + 15 :]
        part, half = da.shape[0], g1a.shape[0]
        cut = half + g2a.shape[0]
        block = gather_blocks(refs[: len(inputs)], blocks)
        table = gather_blocks(refs[len(inputs) : count], tables)
        own = lax.axis_index("sp")
        scale = scale_of(table, own, experts)
        hidden = []
        for i in range(0, hidden_size, 2 * part):
            g = dot(block, gate_ref[:, i : i + 2 * part])
            u = dot(block, up_ref[:, i : i + 2 * part])
            hidden.append((silu(g) * u * scale).astype(bf16))
        scale = scale_of(table, own ^ 1, experts)
        rest = []
        for i, top in enumerate((g1a, g1b, g1c, g1d)):
            side = (i % 2) * 2 * part
            gu = dot(block[:, :half], top[...])
            gu += dot(block[:, half:cut], (g2a, g2c)[i // 2][:, side : side + 2 * part])
            gu += dot(block[:, cut:], (g3a, g3c)[i // 2][:, side : side + 2 * part])
            rest.append((silu(gu[:, :part]) * gu[:, part:] * scale).astype(bf16))
        hidden.append(jnp.concatenate(rest[:2], 1))
        hidden.append(jnp.concatenate(rest[2:], 1))
        step = 512
        for n in range(0, width, step):
            cols = slice(n, n + step)
            total = dot(hidden[0], down_ref[0 : 2 * part, cols])
            total += dot(hidden[1], down_ref[2 * part : 4 * part, cols])
            total += dot(hidden[2], jnp.concatenate([da[:, cols], db[:, cols]], 0))
            total += dot(hidden[3], jnp.concatenate([dc[:, cols], dd[:, cols]], 0))
            total = total.astype(bf16)
            piece, start = n // (width // PIECES), n % (width // PIECES)
            for i in range(len(blocks)):
                out = outs[PIECES * i + piece]
                out[:, start : start + step] = total[i * rows : (i + 1) * rows]
            if sends and n < width // 2:
                rest = block[:, n + width // 2 : n + width // 2 + step]
                outs[-2][:, cols] = jnp.where(in_middle(), rest, total)
            elif sends:
                outs[-1][:, n - width // 2 : n - width // 2 + step] = total

    flops = 12 * len(blocks) * rows * width * hidden_size
    shapes = [((rows, width // PIECES), bf16)] * (PIECES * len(blocks))
    if sends:
        shapes += [((rows, width // 2), bf16)] * 2
    operands = [*inputs, *inputs_t, gate, up, down, *others]
    limit = 4 + 6 * len(blocks)
    return call(kernel, shapes, *operands, limit=limit, flops=flops)


def layer(*args):
    return dense_body(*args)


def solution(mesh):
    few = mesh.shape["sp"] == 8 and mesh.shape["tp"] == 4
    return jax.shard_map(
        layer if few else routed_body,
        mesh=mesh,
        in_specs=(
            P("sp", "tp"),
            P("sp", "tp"),
            P("sp", "tp"),
            P(None, "tp"),
            P("tp", None),
            P(),
            P(("sp", "tp"), None),
            P(),
            P("sp", None, None),
            P("sp", None, None),
            P("sp", None, None),
            P(),
            P(),
            P(),
            P(),
            P(("sp", "tp"), None),
            P(("sp", "tp"), None),
        ),
        out_specs=P(("sp", "tp"), None),
        check_vma=False,
    )
```
